32 devices in a mesh: grp: 2 (over y), sp: 4 (over z), tp: 4 (over x, core).
Axes of the slice: x: 2, y: 2, z: 4, core: 2. Of those that a mesh axis runs over, the one named last changes fastest.
Arguments:
- latent: bfloat16 [2048, 2048], P(('grp', 'sp', 'tp')), parts along dimension 0, may hold values from -6 to 6
- cond: bfloat16 [4096], P(('grp', 'sp')), parts along dimension 0, may hold values from -6 to 6
- context: bfloat16 [512, 2048], P(('grp', 'sp')), parts along dimension 0, may hold values from -6 to 6
- context_cond: bfloat16 [2048], P('sp'), may hold values from -6 to 6
- norm_gain: bfloat16 [2048], replicated, may hold values from 0.099609375 to 1.8984375
- mod_shift: bfloat16 [2048, 2048], P('sp', 'tp'), may hold values from -0.125 to 0.125
- mod_scale: bfloat16 [2048, 2048], P('sp', 'tp'), may hold values from -0.125 to 0.125
- mod_gate: bfloat16 [2048, 2048], P('sp', 'tp'), may hold values from -0.125 to 0.125
- w_query: bfloat16 [2048, 2048], P(None, 'tp'), may hold values from -0.125 to 0.125
- w_key: bfloat16 [2048, 2048], P(None, 'tp'), may hold values from -0.125 to 0.125
- w_value: bfloat16 [2048, 4096], P(None, 'tp'), may hold values from -0.125 to 0.125
- w_gate: bfloat16 [2048, 4096], P(None, 'tp'), may hold values from -0.125 to 0.125
- w_out: bfloat16 [4096, 2048], P('tp'), may hold values from -0.09375 to 0.09375
- decay_rate: float32 [2, 8], P(None, 'tp'), may hold values from 0.00015625 to 0.034
- context_gain: float32 [8], P('tp'), may hold values from 3 to 10
Outputs:
- mixed: bfloat16 [2048, 2048], P(('grp', 'sp', 'tp')), parts along dimension 0
The draws below stay inside these ranges and needn't reach their ends.
There are 2 independent parts, one for each index of `grp`. The reference program is written for one: setup_inputs(seed, part) draws one part's arguments, and reference() takes and returns one part's arrays. A program takes and returns all parts, laid end to end along the dimension named above; an argument that names none is the same for every part. Nothing has to cross between parts.
All inputs are finite; a program needn't handle non-finite values.
Results may differ from the reference program's by a relative error of at most 0.009.
Values may be sent and summed in bfloat16 or wider, within the bound.
A program may use at most 128 MiB of HBM per device.

```python
import math
import jax
import jax.numpy as jnp
from jax import lax

D = 2048
H = 8
DK = 256
DV = 512
GRID_W = 128
BLOCK = 128
NL = 1024
CTX = 256
N_TP = 4


def draw_decay_rate(key, part):
    base = jax.random.fold_in(key, 17)
    pick_key, fast_key, slow_key = jax.random.split(base, 3)
    share = 0.5
    fast = jax.random.uniform(pick_key, (2, H), jnp.float32) < share
    fast_rate = jnp.exp(jax.random.uniform(fast_key, (2, H), jnp.float32, math.log(1.0 / 100.0), math.log(1.0 / 30.0)))
    slow_rate = jnp.exp(jax.random.uniform(slow_key, (2, H), jnp.float32, math.log(0.2), math.log(2.0))) / (NL + CTX)
    return jnp.where(fast, fast_rate, slow_rate).astype(jnp.float32)


def level_of(rng, extent, cuts, low, high):
    factor_of = 1.0
    for position, shards_of in cuts:
        heights = jax.random.uniform(jax.random.fold_in(jax.random.fold_in(rng, 6), position), (shards_of,), jnp.float32, low / len(cuts), high / len(cuts))
        factor_of = factor_of * jnp.repeat(jnp.exp(heights), extent[position] // shards_of).reshape((-1,) + (1,) * (len(extent) - 1 - position))
    return factor_of


def gaussian(key, shape, scale, reach, cuts=(), kind=jnp.bfloat16):
    entries = scale * jax.random.normal(key, shape, jnp.float32)
    if cuts:
        entries = entries * level_of(key, shape, cuts, -0.22, 0.18)
    return jnp.clip(entries, -reach, reach).astype(kind)


def setup_inputs(seed: int = 0, part: int = 0) -> dict:
    arg_keys = jax.random.split(jax.random.key(seed), 16)
    own_keys = jax.random.split(jax.random.fold_in(arg_keys[15], part), 16)
    latent = gaussian(own_keys[0], (NL, D), 1.0, 6.0, ((0, 16),))
    cond = gaussian(own_keys[1], (D,), 1.0, 6.0, ((0, 4),))
    context = gaussian(own_keys[2], (CTX, D), 1.0, 6.0, ((0, 4),))
    context_cond = gaussian(arg_keys[3], (D,), 1.0, 6.0, ((0, 4),))
    norm_gain = jnp.clip(1.0 + 0.18 * jax.random.normal(arg_keys[4], (D,), jnp.float32), 0.099609375, 1.8984375).astype(jnp.bfloat16)
    mod_shift = gaussian(arg_keys[5], (D, D), D ** -0.5, 0.125, ((0, 4), (1, 4)))
    mod_scale = gaussian(arg_keys[6], (D, D), D ** -0.5, 0.125, ((0, 4), (1, 4)))
    mod_gate = gaussian(arg_keys[7], (D, D), D ** -0.5, 0.125, ((0, 4), (1, 4)))
    w_query = gaussian(arg_keys[8], (D, H * DK), D ** -0.5, 0.125, ((1, 4),))
    w_key = gaussian(arg_keys[9], (D, H * DK), D ** -0.5, 0.125, ((1, 4),))
    w_value = gaussian(arg_keys[10], (D, H * DV), D ** -0.5, 0.125, ((1, 4),))
    w_gate = gaussian(arg_keys[11], (D, H * DV), D ** -0.5, 0.125, ((1, 4),))
    w_out = gaussian(arg_keys[12], (H * DV, D), (H * DV) ** -0.5, 0.09375, ((0, 4),))
    decay_rate = draw_decay_rate(jax.random.fold_in(arg_keys[15], 71), part)
    context_gain = jnp.clip(jnp.exp(math.log(10.0) - 1.2039728 * jax.random.uniform(arg_keys[14], (H,), jnp.float32) ** level_of(arg_keys[14], (H,), ((0, 4),), -0.2, 0.2)), 3.0, 10.0)
    return {"latent": latent, "cond": cond, "context": context, "context_cond": context_cond, "norm_gain": norm_gain, "mod_shift": mod_shift, "mod_scale": mod_scale, "mod_gate": mod_gate, "w_query": w_query, "w_key": w_key, "w_value": w_value, "w_gate": w_gate, "w_out": w_out, "decay_rate": decay_rate, "context_gain": context_gain}


norm_eps = 1e-06
rope_base = 10000.0
highest = lax.Precision.HIGHEST

def modulated(rows, norm_gain, shift, scale):
    values = rows.astype(jnp.float32)
    normed = values * lax.rsqrt(lax.optimization_barrier(jnp.mean(values * values, axis=-1, keepdims=True)) + norm_eps)
    return (normed * norm_gain.astype(jnp.float32) * (1.0 + scale) + shift).astype(jnp.bfloat16)

def rotate(vectors, positions):
    depth = vectors.shape[-1]
    freqs = depth // 4
    inv_freq = rope_base ** (-jnp.arange(freqs, dtype=jnp.float32) / freqs)
    grid_row = (positions // GRID_W).astype(jnp.float32)
    grid_col = (positions % GRID_W).astype(jnp.float32)
    angles = jnp.concatenate([grid_row[:, None] * inv_freq, grid_col[:, None] * inv_freq], axis=-1)[:, None, :]
    cos_table = jnp.cos(angles)
    sin_table = jnp.sin(angles)
    first_half, second_half = jnp.split(vectors, 2, axis=-1)
    return jnp.concatenate([first_half * cos_table - second_half * sin_table, second_half * cos_table + first_half * sin_table], axis=-1)

def rounded(values):
    return lax.optimization_barrier(values.astype(jnp.bfloat16)).astype(jnp.float32)

def context_states(ctx_key, ctx_value, fwd_rate, bwd_rate, context_gain):
    total = ctx_key.shape[0]
    place = jnp.arange(total, dtype=jnp.float32)[:, None]
    fwd_weight = jnp.exp(-fwd_rate[None, :] * (total - 1.0 - place))
    bwd_weight = jnp.exp(-bwd_rate[None, :] * place)
    keys_f = lax.optimization_barrier(ctx_key).astype(jnp.float32)
    values_f = lax.optimization_barrier(ctx_value).astype(jnp.float32)
    fwd_keys = rounded(keys_f * fwd_weight[:, :, None])
    bwd_keys = rounded(keys_f * bwd_weight[:, :, None])
    fwd_state = jnp.einsum('jhd,jhe->hde', fwd_keys, values_f, precision=highest)
    bwd_state = jnp.einsum('jhd,jhe->hde', bwd_keys, values_f, precision=highest)
    return (fwd_state * context_gain[:, None, None], bwd_state * context_gain[:, None, None])

def reference(latent, cond, context, context_cond, norm_gain, mod_shift, mod_scale, mod_gate, w_query, w_key, w_value, w_gate, w_out, decay_rate, context_gain):
    cond_rows = jax.nn.silu(jnp.stack([cond, context_cond]).astype(jnp.float32)).astype(jnp.bfloat16)
    shift = jnp.dot(cond_rows, mod_shift, preferred_element_type=jnp.float32)
    scale = jnp.dot(cond_rows, mod_scale, preferred_element_type=jnp.float32)
    gate = jnp.dot(cond_rows[0:1], mod_gate, preferred_element_type=jnp.float32)
    h_latent = modulated(latent, norm_gain, shift[0], scale[0])
    h_context = modulated(context, norm_gain, shift[1], scale[1])
    positions = jnp.arange(NL, dtype=jnp.int32)
    query = rotate(jnp.dot(h_latent, w_query, preferred_element_type=jnp.float32).reshape(NL, H, DK), positions).astype(jnp.bfloat16)
    keys = rotate(jnp.dot(h_latent, w_key, preferred_element_type=jnp.float32).reshape(NL, H, DK) * DK ** (-0.5), positions).astype(jnp.bfloat16)
    values = jnp.dot(h_latent, w_value, preferred_element_type=jnp.float32).astype(jnp.bfloat16).reshape(NL, H, DV)
    gate_pre = jnp.dot(h_latent, w_gate, preferred_element_type=jnp.float32).reshape(NL, H, DV)
    ctx_key = (jnp.dot(h_context, w_key, preferred_element_type=jnp.float32) * DK ** (-0.5)).astype(jnp.bfloat16)
    ctx_value = jnp.dot(h_context, w_value, preferred_element_type=jnp.float32).astype(jnp.bfloat16)
    fwd_rate = decay_rate[0]
    bwd_rate = decay_rate[1]
    ctx_fwd, ctx_bwd = context_states(ctx_key.reshape(CTX, H, DK), ctx_value.reshape(CTX, H, DV), fwd_rate, bwd_rate, context_gain)
    blocks = NL // BLOCK
    query_f = lax.optimization_barrier(query).astype(jnp.float32).reshape(blocks, BLOCK, H, DK)
    keys_f = lax.optimization_barrier(keys).astype(jnp.float32).reshape(blocks, BLOCK, H, DK)
    values_f = lax.optimization_barrier(values).astype(jnp.float32).reshape(blocks, BLOCK, H, DV)
    place = jnp.arange(BLOCK, dtype=jnp.float32)
    gap = place[:, None] - place[None, :]
    mask = jnp.where(gap >= 0, jnp.exp(-fwd_rate[:, None, None] * jnp.maximum(gap, 0.0)), 0.0) + jnp.where(gap <= 0, jnp.exp(-bwd_rate[:, None, None] * jnp.maximum(-gap, 0.0)), 0.0)
    scores = jnp.einsum('bihd,bjhd->bhij', query_f, keys_f, precision=highest)
    weights = lax.optimization_barrier((scores * mask[None]).astype(jnp.bfloat16)).astype(jnp.float32)
    retained = jnp.einsum('bhij,bjhe->bihe', weights, values_f, precision=highest)
    fwd_qw = jnp.exp(-fwd_rate[None, :] * (place[:, None] + 1.0))
    bwd_qw = jnp.exp(-bwd_rate[None, :] * (BLOCK - place[:, None]))
    fwd_kw = jnp.exp(-fwd_rate[None, :] * (BLOCK - 1.0 - place[:, None]))
    bwd_kw = jnp.exp(-bwd_rate[None, :] * place[:, None])
    fwd_keys = rounded(keys_f * fwd_kw[None, :, :, None])
    bwd_keys = rounded(keys_f * bwd_kw[None, :, :, None])
    fwd_step_decay = jnp.exp(-fwd_rate * BLOCK)[:, None, None]
    bwd_step_decay = jnp.exp(-bwd_rate * BLOCK)[:, None, None]

    def fwd_step(state, block):
        block_query, block_keys, block_values = block
        cross = jnp.einsum('ihd,hde->ihe', block_query, rounded(state), precision=highest) * fwd_qw[:, :, None]
        added = jnp.einsum('jhd,jhe->hde', block_keys, block_values, precision=highest)
        return (fwd_step_decay * state + added, cross)

    def bwd_step(state, block):
        block_query, block_keys, block_values = block
        cross = jnp.einsum('ihd,hde->ihe', block_query, rounded(state), precision=highest) * bwd_qw[:, :, None]
        added = jnp.einsum('jhd,jhe->hde', block_keys, block_values, precision=highest)
        return (bwd_step_decay * state + added, cross)
    fwd_final, fwd_cross = lax.scan(fwd_step, ctx_fwd, (query_f, fwd_keys, values_f))
    bwd_final, bwd_cross = lax.scan(bwd_step, ctx_bwd, (query_f, bwd_keys, values_f), reverse=True)
    retained = (retained + fwd_cross + bwd_cross).reshape(NL, H, DV)
    centre = lax.optimization_barrier(jnp.mean(retained, axis=-1, keepdims=True))
    variance = lax.optimization_barrier(jnp.mean(jnp.square(retained - centre), axis=-1, keepdims=True))
    normed = (retained - centre) * lax.rsqrt(variance + norm_eps)
    gated = (jax.nn.silu(gate_pre) * normed).astype(jnp.bfloat16).reshape(NL, H * DV)
    group_cols = H // N_TP * DV
    total = jnp.zeros((NL, D), jnp.float32)
    for group in range(N_TP):
        lower = group * group_cols
        partial_sum = jnp.dot(gated[:, lower:lower + group_cols], w_out[lower:lower + group_cols], preferred_element_type=jnp.float32).astype(jnp.bfloat16)
        total = total + lax.optimization_barrier(partial_sum).astype(jnp.float32)
    return (latent.astype(jnp.float32) + gate[0] * total).astype(jnp.bfloat16)
```

```python
import functools
import math
from types import SimpleNamespace

import jax
import jax.numpy as jnp
from jax import lax
from jax.experimental import pallas as pl
from jax.experimental.pallas import tpu as pltpu
from jax.sharding import PartitionSpec as P

DK = 256
GRID_W = 128
TILE = 256
PIECE = 16
CHUNK = 32
LAG = 5
PRE = 3
NC = 4
norm_eps = 1e-06
rope_base = 10000.0
MESH = pl.DeviceIdType.MESH
F32, BF16 = jnp.float32, jnp.bfloat16


def dot(a, b):
    return jnp.dot(a, b, preferred_element_type=F32)


def dot_tn(a, b):
    return lax.dot_general(a, b, (((0,), (0,)), ((), ())), preferred_element_type=F32)


def dot_nt(a, b):
    return lax.dot_general(a, b, (((1,), (1,)), ((), ())), preferred_element_type=F32)


def remote(src, dst, send, recv, where):
    return pltpu.make_async_remote_copy(
        src_ref=src, dst_ref=dst, send_sem=send, recv_sem=recv, device_id=where, device_id_type=MESH
    )


def rows_of(start, size):
    return pl.ds(pl.multiple_of(start, size), size)


def cols(j, size):
    return pl.ds(pl.multiple_of(j * size, size), size)


def tiled(x, count):
    return jnp.concatenate([x] * count, axis=0) if count > 1 else x


def kernel(S, T, names, *refs):
    (
        latent,
        cond,
        context_cond,
        context,
        norm_gain,
        mod_shift,
        mod_scale,
        mod_gate,
        w_query,
        w_key,
        w_value,
        w_gate,
        w_out,
        decay_in,
        gain_in,
        out,
    ) = refs[:16]
    r = SimpleNamespace(**dict(zip(names, refs[16:])))

    sp, tp = lax.axis_index("sp"), lax.axis_index("tp")
    R, D = latent.shape
    Cr = context.shape[0]
    half = Cr // 2
    CT = Cr * S
    span = R * T
    nh = w_query.shape[1] // DK
    DV = w_value.shape[1] // nh
    Mr, Mc = mod_shift.shape
    G, GD = Mc // 128, D // 128
    X = T // 2
    pieces = R // PIECE
    chip, core = tp // 2, lax.rem(tp, 2)
    partner = tp + 1 - 2 * core
    is_end = jnp.logical_or(sp == 0, sp == S - 1)
    W = D // NC
    per_head = DK // CHUNK
    n = nh * per_head
    hop = (sp, S - 1 - sp)
    after = (sp + 1, sp - 1)
    before = (sp - 1, sp + 1)
    sp_peers = [lax.rem(sp + k, S) for k in range(1, S)]
    others = [lax.rem(chip + k, X) for k in range(1, X)]
    peers = [
        (lax.rem(sp + i, S), lax.rem(tp + j, T)) for i in range(S) for j in range(T) if i or j
    ]

    barrier = pltpu.get_barrier_semaphore()
    for a, b in peers:
        pl.semaphore_signal(
            barrier, inc=1, device_id={"sp": a, "tp": b}, device_id_type=MESH
        )

    own = rows_of(tp * R, R)
    pairs = [
        (cond, r.cond),
        (context_cond, r.ccond),
        (mod_shift, r.m_shift),
        (mod_scale, r.m_scale),
        (latent, r.x_all.at[own]),
        (mod_gate, r.m_gate),
        (decay_in, r.decay),
        (gain_in, r.gain),
        (norm_gain, r.ngain),
        (context, r.c_all.at[rows_of(sp * Cr, Cr)]),
        (w_key, r.vk),
        (w_value, r.vv),
        (w_query, r.vq),
        (w_gate, r.vg),
        (w_out, r.vo),
    ]
    loads = [
        pltpu.make_async_copy(src, dst, r.load_sem.at[i]) for i, (src, dst) in enumerate(pairs)
    ]
    for copy in loads:
        copy.start()

    for copy in loads[:2]:
        copy.wait()

    def silu_row(ref):
        v = ref[...].astype(F32)
        v = v / (1.0 + jnp.exp(-v))
        return jnp.concatenate([v[g : g + 1, :] for g in range(Mr // 128)], axis=1)

    rows = jnp.concatenate(
        [silu_row(r.cond), silu_row(r.ccond), jnp.zeros((14, Mr), F32)], axis=0
    ).astype(BF16)
    loads[2].wait()
    shift_part = dot(rows, r.m_shift[...])
    loads[3].wait()
    scale_part = dot(rows, r.m_scale[...])

    def lanes(x, row, g):
        return x[row : row + 1, g * 128 : (g + 1) * 128]

    for g in range(G):
        r.m1[sp, tp, g : g + 1, :] = lanes(shift_part, 0, g)
        r.m1[sp, tp, G + g : G + g + 1, :] = lanes(scale_part, 0, g)

    def m1_copy(owner, to, k):
        slot = r.m1.at[owner[0], owner[1]]
        return remote(slot, slot, r.m1_send.at[k], r.m1_recv.at[k], {"sp": to[0], "tp": to[1]})

    def m2_copy(owner, to, k):
        slot = r.m2.at[owner[0], owner[1]]
        return remote(slot, slot, r.m2_send.at[k], r.m2_recv.at[k], {"sp": to[0], "tp": to[1]})

    def lat_copy(owner, p, to, which):
        place = rows_of(owner * R + p * PIECE, PIECE)
        return remote(
            r.x_all.at[place],
            r.x_all.at[place],
            r.lat_send.at[which, to if which == 0 else owner, p],
            r.lat_recv.at[owner, p],
            {"tp": to},
        )

    def ctx_copy(owner, part_core, send, recv, where):
        place = rows_of(owner * Cr + part_core * half, half)
        return remote(r.c_all.at[place], r.c_all.at[place], send, recv, where)

    def ctx_out(to):
        return ctx_copy(sp, core, r.ctx_send.at[to], r.ctx_recv.at[0, sp], {"sp": to})

    loads[4].wait()
    pl.semaphore_wait(barrier, len(peers))

    for k, to in enumerate(peers):
        m1_copy((sp, tp), to, k).start()
    for p in range(pieces):
        for o in others:
            lat_copy(tp, p, 2 * o + core, 0).start()
    for p in range(pieces):
        lat_copy(tp, p, partner, 0).start()

    gate_wait = loads[5]
    gate_wait.wait()
    gate_part = dot(rows, r.m_gate[...])
    for g in range(G):
        r.m2[sp, tp, g : g + 1, :] = lanes(shift_part, 1, g)
        r.m2[sp, tp, G + g : G + g + 1, :] = lanes(scale_part, 1, g)
        r.m2[sp, tp, 2 * G + g : 2 * G + g + 1, :] = lanes(gate_part, 0, g)
    loads[9].wait()
    for k, to in enumerate(peers):
        m2_copy((sp, tp), to, k).start()
    for to in sp_peers:
        ctx_out(to).start()

    F = DK // 4
    pos = (lax.broadcasted_iota(jnp.int32, (span, 2 * F), 0) + sp * span).astype(F32)
    lane = lax.broadcasted_iota(jnp.int32, (span, 2 * F), 1)
    grid_row = jnp.floor(pos * (1.0 / GRID_W))
    grid_col = pos - grid_row * GRID_W
    freq = jnp.where(lane < F, lane, lane - F).astype(F32)
    angle = jnp.where(lane < F, grid_row, grid_col) * jnp.exp(freq * (-math.log(rope_base) / F))
    r.cos_t[...] = jnp.cos(angle)
    r.sin_t[...] = jnp.sin(angle)

    for copy in loads[6:9]:
        copy.wait()

    def decay_tables(h, _):
        a, b = r.decay[0, h], r.decay[1, h]
        place = lax.broadcasted_iota(jnp.int32, (span, 128), 0).astype(F32)
        r.ktab[0, h] = jnp.exp(-a * (span - 1.0 - place))
        r.ktab[1, h] = jnp.exp(-b * place)
        r.qtab[0, h] = jnp.exp(-a * (place + 1.0))
        r.qtab[1, h] = jnp.exp(-b * (span - place))
        far = lax.broadcasted_iota(jnp.int32, (CT, 128), 0).astype(F32)
        r.ctab[0, h] = jnp.exp(-a * (CT - 1.0 - far))
        r.ctab[1, h] = jnp.exp(-b * far)
        for d, rate in enumerate((a, b)):
            r.fade[d, h] = jnp.exp(jnp.full((8, DV), -rate * span, F32))
        gap = (
            lax.broadcasted_iota(jnp.int32, (span, span), 0)
            - lax.broadcasted_iota(jnp.int32, (span, span), 1)
        ).astype(F32)
        mask = jnp.where(gap >= 0, jnp.exp(-a * jnp.maximum(gap, 0.0)), 0.0)
        mask += jnp.where(gap <= 0, jnp.exp(-b * jnp.maximum(-gap, 0.0)), 0.0)
        r.mask[h] = mask
        return 0

    lax.fori_loop(0, nh, decay_tables, 0)

    def stat(src, dst, start, count):
        place = rows_of(start, count)
        x = src[place, :].astype(F32)
        inv = lax.rsqrt(jnp.mean(x * x, axis=-1, keepdims=True) + norm_eps)
        dst[place, :] = jnp.broadcast_to(inv, (count, 128))

    def apply(src, dst, inv, start, count, row):
        place = rows_of(start, count)
        scale = inv[place, :]
        for j in range(GD):
            c = slice(j * 128, (j + 1) * 128)
            mult = tiled(r.mult[row, :, c], count // 8)
            shift = tiled(r.shift[row, :, c], count // 8)
            dst[place, c] = (src[place, c].astype(F32) * scale * mult + shift).astype(BF16)

    def spread(row, source, at_shift, at_scale):
        for t in range(T):
            total = source[0, t]
            for s in range(1, S):
                total = total + source[s, t]
            r.g16[0, t * G : (t + 1) * G, :] = total[at_shift : at_shift + G]
            r.g16[1, t * G : (t + 1) * G, :] = total[at_scale : at_scale + G]
            if row:
                r.g16[2, t * G : (t + 1) * G, :] = total[2 * G : 3 * G]
        r.g16[1] = r.ngain[...].astype(F32) * (1.0 + r.g16[1])
        for j in range(GD):
            c = slice(j * 128, (j + 1) * 128)
            r.shift[row, :, c] = jnp.broadcast_to(r.g16[0, j : j + 1, :], (8, 128))
            r.mult[row, :, c] = jnp.broadcast_to(r.g16[1, j : j + 1, :], (8, 128))
            if row:
                r.gate[:, c] = jnp.broadcast_to(r.g16[2, j : j + 1, :], (8, 128))

    stat(r.x_all, r.inv, tp * R, R)
    for p in range(pieces - 1):
        for o in others:
            lat_copy(2 * o + core, p, tp, 0).wait_recv()
            lat_copy(2 * o + core, p, partner, 1).start()
    opposite = [(lax.rem(sp - i + S, S), lax.rem(tp - j + T, T)) for i in range(S) for j in range(T) if i or j]
    for k, (a, b) in enumerate(opposite):
        m1_copy((a, b), (a, b), k).wait_recv()
    spread(0, r.m1, 0, G)
    apply(r.x_all, r.h, r.inv, tp * R, R, 0)
    for o in others:
        lat_copy(2 * o + core, pieces - 1, tp, 0).wait_recv()
        lat_copy(2 * o + core, pieces - 1, partner, 1).start()
        stat(r.x_all, r.inv, (2 * o + core) * R, R)
        apply(r.x_all, r.h, r.inv, (2 * o + core) * R, R, 0)
    for p in range(pieces):
        lat_copy(partner, p, partner, 0).wait_recv()
    stat(r.x_all, r.inv, partner * R, R)
    apply(r.x_all, r.h, r.inv, partner * R, R, 0)
    for o in others:
        owner = 2 * o + 1 - core
        for p in range(pieces):
            lat_copy(owner, p, owner, 0).wait_recv()
        stat(r.x_all, r.inv, owner * R, R)
        apply(r.x_all, r.h, r.inv, owner * R, R, 0)

    scale_k = DK**-0.5

    def rotated(x):
        u, w = x[:, : DK // 2], x[:, DK // 2 :]
        c, s = r.cos_t[...], r.sin_t[...]
        return jnp.concatenate([u * c - w * s, w * c + u * s], axis=1).astype(BF16)

    def st_copy(d, c, to):
        place = rows_of(c * CHUNK, CHUNK)
        return remote(
            r.st_out.at[d, place],
            r.st_in.at[d, place],
            r.st_send.at[d, c],
            r.st_recv.at[d, c],
            {"sp": to},
        )

    loads[10].wait()
    loads[11].wait()
    first = jnp.where(2 * sp < S, 0, 1)
    onward = jnp.where(2 * sp < S, sp + 1, sp - 1)

    def wide(x):
        return jnp.concatenate([x] * (DK // 128), axis=1)

    def head_kv(h, _):
        k = rotated(dot(r.h[...], r.vk[:, cols(h, DK)]) * scale_k)
        r.k[h] = k
        v = dot(r.h[...], r.vv[:, cols(h, DV)]).astype(BF16)
        r.v[:, cols(h, DV)] = v
        kf = k.astype(F32)
        r.loc[first, cols(h, DK), :] = dot_tn((kf * wide(r.ktab[first, h])).astype(BF16), v)

        @pl.when(is_end)
        def _():
            for c in range(per_head):
                place = rows_of(h * DK + c * CHUNK, CHUNK)
                r.st_out[first, place, :] = r.loc[first, place, :].astype(BF16)
                st_copy(first, h * per_head + c, onward).start()

        r.loc[1 - first, cols(h, DK), :] = dot_tn(
            (kf * wide(r.ktab[1 - first, h])).astype(BF16), v
        )
        return 0

    lax.fori_loop(0, nh, head_kv, 0)

    def relay(d, c):
        st_copy(d, c, before[d]).wait_recv()
        place = rows_of(c * CHUNK, CHUNK)
        fade = r.fade[d, lax.div(c, per_head), 0:1, :]
        r.st_out[d, place, :] = (
            r.st_in[d, place, :].astype(F32) * fade + r.loc[d, place, :]
        ).astype(BF16)
        st_copy(d, c, after[d]).start()

    loads[12].wait()
    q_all = dot(r.h[...], r.vq[...])
    for h in range(nh):
        q = rotated(q_all[:, h * DK : (h + 1) * DK])
        r.q[h] = q
        qf = q.astype(F32)
        r.qab[h, :, :DK] = (qf * wide(r.qtab[0, h])).astype(BF16)
        r.qab[h, :, DK:] = (qf * wide(r.qtab[1, h])).astype(BF16)
    loads[13].wait()
    loads[14].wait()

    def gate_item(j):
        pre = dot(r.h[...], r.vg[:, cols(j, TILE)])
        r.g[:, cols(j, TILE)] = pre / (1.0 + jnp.exp(-pre))

    def within_item(h):
        weights = (dot_nt(r.q[h], r.k[h]) * r.mask[h]).astype(BF16)
        r.ret[h] = dot(weights, r.v[:, cols(h, DV)])

    def ctx_forward_item(_):
        for p in sp_peers:
            ctx_copy(p, core, r.ctx_send.at[p], r.ctx_recv.at[0, p], {"sp": p}).wait_recv()
            ctx_copy(p, core, r.ctx_fsend.at[p], r.ctx_recv.at[1, p], {"tp": partner}).start()
        for k, (a, b) in enumerate(opposite):
            m2_copy((a, b), (a, b), k).wait_recv()
        spread(1, r.m2, 0, G)

    def ctx_arrive_item(_):
        for p in sp_peers:
            ctx_copy(
                p, 1 - core, r.ctx_fsend.at[p], r.ctx_recv.at[1, p], {"tp": partner}
            ).wait_recv()

    def ctx_norm_item(j):
        stat(r.c_all, r.cinv, j * 64, 64)
        apply(r.c_all, r.hc, r.cinv, j * 64, 64, 1)

    M = min(CT, TILE)

    def ctx_key_item(j):
        place, h = rows_of(lax.div(j, nh) * M, M), lax.rem(j, nh)
        r.ck[h, place, :] = (dot(r.hc[place, :], r.vk[:, cols(h, DK)]) * scale_k).astype(BF16)

    nv = nh * DV // TILE

    def ctx_value_item(j):
        place, t = rows_of(lax.div(j, nv) * M, M), lax.rem(j, nv)
        r.cv[place, cols(t, TILE)] = dot(r.hc[place, :], r.vv[:, cols(t, TILE)]).astype(BF16)

    def ctx_state_item(j):
        h, d = lax.div(j, 2), lax.rem(j, 2)
        keys = (r.ck[h].astype(F32) * wide(r.ctab[d, h])).astype(BF16)
        away = jnp.where(d == 0, hop[0], hop[1]).astype(F32) * span
        weight = jnp.exp(jnp.full((1, DV), -r.decay[d, h] * away, F32)) * r.gain[h]
        r.base[d, cols(h, DK), :] = dot_tn(keys, r.cv[:, cols(h, DV)]) * weight

    items = [
        (nv, gate_item),
        (1, ctx_forward_item),
        (nh, within_item),
        (1, ctx_arrive_item),
        (CT // 64, ctx_norm_item),
        (CT // M * nh, ctx_key_item),
        (CT // M * nv, ctx_value_item),
        (2 * nh, ctx_state_item),
    ]
    total_items = sum(count for count, _ in items)
    inner = jnp.logical_not(is_end)

    def lap(i, _):
        for d in range(2):
            c = i - PRE - LAG * (hop[d] - 1)

            @pl.when(jnp.logical_and(inner, jnp.logical_and(c >= 0, c < n)))
            def _():
                relay(d, c)

        start = 0
        for count, run in items:

            @pl.when(jnp.logical_and(i >= start, i < start + count))
            def _():
                run(i - start)

            start += count
        return 0

    lax.fori_loop(0, max(PRE + n + LAG * max(S - 3, 0), total_items), lap, 0)

    def project(h, start, count, c):
        return dot(r.gated[h, rows_of(start, count), :], r.vo[h * DV : (h + 1) * DV, cols(c, W)])

    for h in range(nh):
        for d in range(2):

            @pl.when(hop[d] == 0)
            def _():
                r.ent[h, d * DK : (d + 1) * DK, :] = r.base[d, h * DK : (h + 1) * DK, :].astype(
                    BF16
                )

            @pl.when(hop[d] > 0)
            def _():
                def enter(c, _):
                    @pl.when(hop[d] == S - 1)
                    def _():
                        st_copy(d, h * per_head + c, before[d]).wait_recv()

                    place = rows_of(h * DK + c * CHUNK, CHUNK)
                    r.ent[h, rows_of(d * DK + c * CHUNK, CHUNK), :] = (
                        r.st_in[d, place, :].astype(F32) + r.base[d, place, :]
                    ).astype(BF16)
                    return 0

                lax.fori_loop(0, per_head, enter, 0)

        ret = r.ret[h] + dot(r.qab[h], r.ent[h])
        ret = ret - jnp.mean(ret, axis=-1, keepdims=True)
        ret = ret * lax.rsqrt(jnp.mean(ret * ret, axis=-1, keepdims=True) + norm_eps)
        r.gated[h] = (r.g[:, h * DV : (h + 1) * DV] * ret).astype(BF16)
        if h < nh - 1:

            def gather(c, _):
                value = project(h, 0, span, c)
                if h:
                    value = value + r.acc[:, cols(c, W)]
                r.acc[:, cols(c, W)] = value
                return 0

            lax.fori_loop(0, NC, gather, 0)

    def chip_rows(c, o):
        value = project(nh - 1, 2 * o * R, 2 * R, c)
        if nh > 1:
            value = value + r.acc[rows_of(2 * o * R, 2 * R), cols(c, W)]
        value = value.astype(BF16)
        r.part[c, 2 * o] = value[:R]
        r.part[c, 2 * o + 1] = value[R:]

    def p1_copy(c, o):
        return remote(
            r.part.at[c, 2 * o + 1 - core],
            r.p1.at[c, o],
            r.p1_send.at[c, o],
            r.p1_recv.at[c, o],
            {"tp": partner},
        )

    def p2_copy(c):
        return remote(
            r.part.at[c, partner], r.p2.at[c], r.p2_send.at[c], r.p2_recv.at[c], {"tp": partner}
        )

    def x_copy(c, owner, o):
        return remote(
            r.xs.at[c, o],
            r.xr.at[c, owner],
            r.x_send.at[c, o],
            r.x_recv.at[c, owner],
            {"tp": 2 * o + core},
        )

    def away(c, _):
        for o in others:
            chip_rows(c, o)
            p1_copy(c, o).start()
        return 0

    lax.fori_loop(0, NC, away, 0)

    def across(c, _):
        for o in others:
            p1_copy(c, o).wait_recv()
            mine = r.part[c, 2 * o + core].astype(F32)
            r.xs[c, o] = (mine + r.p1[c, o].astype(F32)).astype(BF16)
            x_copy(c, chip, o).start()
        chip_rows(c, chip)
        p2_copy(c).start()
        return 0

    lax.fori_loop(0, NC, across, 0)

    for k in range(len(peers)):
        m1_copy((sp, tp), peers[k], k).wait_send()
        m2_copy((sp, tp), peers[k], k).wait_send()
    for p in range(pieces):
        for o in others:
            lat_copy(tp, p, 2 * o + core, 0).wait_send()
            lat_copy(2 * o + core, p, partner, 1).wait_send()
        lat_copy(tp, p, partner, 0).wait_send()
    for to in sp_peers:
        ctx_out(to).wait_send()
        ctx_copy(to, core, r.ctx_fsend.at[to], r.ctx_recv.at[1, to], {"tp": partner}).wait_send()

    def sent(c, _):
        for d in range(2):

            @pl.when(hop[d] < S - 1)
            def _():
                st_copy(d, c, after[d]).wait_send()

        return 0

    lax.fori_loop(0, n, sent, 0)

    def final(c, _):
        p2_copy(c).wait_recv()
        total = r.part[c, tp].astype(F32) + r.p2[c].astype(F32)
        for o in others:
            x_copy(c, o, o).wait_recv()
            total = total + r.xr[c, o].astype(F32)
        mine = r.x_all[own, cols(c, W)].astype(F32)
        gate = tiled(r.gate[:, cols(c, W)], R // 8)
        out[:, cols(c, W)] = (mine + gate * total).astype(BF16)
        return 0

    lax.fori_loop(0, NC, final, 0)

    def sent_out(c, _):
        for o in others:
            p1_copy(c, o).wait_send()
            x_copy(c, chip, o).wait_send()
        p2_copy(c).wait_send()
        return 0

    lax.fori_loop(0, NC, sent_out, 0)


def body(
    S,
    T,
    latent,
    cond,
    context,
    context_cond,
    norm_gain,
    mod_shift,
    mod_scale,
    mod_gate,
    w_query,
    w_key,
    w_value,
    w_gate,
    w_out,
    decay_rate,
    context_gain,
):
    R, D = latent.shape
    Cr = context.shape[0]
    span, CT = R * T, Cr * S
    nh = w_query.shape[1] // DK
    DV = w_value.shape[1] // nh
    Mr, Mc = mod_shift.shape
    G, GD = Mc // 128, D // 128
    X = T // 2
    W = D // NC
    n = nh * DK // CHUNK
    N = S * T - 1
    pieces = R // PIECE
    v = pltpu.VMEM
    DMA = pltpu.SemaphoreType.DMA
    scratch = dict(
        x_all=v((span, D), BF16),
        c_all=v((CT, D), BF16),
        h=v((span, D), BF16),
        hc=v((CT, D), BF16),
        cond=v((Mr // 128, 128), BF16),
        ccond=v((Mr // 128, 128), BF16),
        ngain=v((GD, 128), BF16),
        decay=pltpu.SMEM(decay_rate.shape, F32),
        gain=pltpu.SMEM(context_gain.shape, F32),
        m_shift=v((Mr, Mc), BF16),
        m_scale=v((Mr, Mc), BF16),
        m_gate=v((Mr, Mc), BF16),
        vq=v(w_query.shape, BF16),
        vk=v(w_key.shape, BF16),
        vv=v(w_value.shape, BF16),
        vg=v(w_gate.shape, BF16),
        vo=v(w_out.shape, BF16),
        m1=v((S, T, 2 * G, 128), F32),
        m2=v((S, T, 3 * G, 128), F32),
        g16=v((3, GD, 128), F32),
        shift=v((2, 8, D), F32),
        mult=v((2, 8, D), F32),
        gate=v((8, D), F32),
        inv=v((span, 128), F32),
        cinv=v((CT, 128), F32),
        cos_t=v((span, DK // 2), F32),
        sin_t=v((span, DK // 2), F32),
        ktab=v((2, nh, span, 128), F32),
        qtab=v((2, nh, span, 128), F32),
        ctab=v((2, nh, CT, 128), F32),
        fade=v((2, nh, 8, DV), F32),
        mask=v((nh, span, span), F32),
        q=v((nh, span, DK), BF16),
        qab=v((nh, span, 2 * DK), BF16),
        k=v((nh, span, DK), BF16),
        v=v((span, nh * DV), BF16),
        ck=v((nh, CT, DK), BF16),
        cv=v((CT, nh * DV), BF16),
        g=v((span, nh * DV), F32),
        ret=v((nh, span, DV), F32),
        gated=v((nh, span, DV), BF16),
        loc=v((2, nh * DK, DV), F32),
        base=v((2, nh * DK, DV), F32),
        st_in=v((2, nh * DK, DV), BF16),
        st_out=v((2, nh * DK, DV), BF16),
        ent=v((nh, 2 * DK, DV), BF16),
        acc=v((span, D), F32),
        part=v((NC, T, R, W), BF16),
        p1=v((NC, X, R, W), BF16),
        p2=v((NC, R, W), BF16),
        xs=v((NC, X, R, W), BF16),
        xr=v((NC, X, R, W), BF16),
        load_sem=DMA((15,)),
        m1_send=DMA((N,)),
        m1_recv=DMA((N,)),
        m2_send=DMA((N,)),
        m2_recv=DMA((N,)),
        lat_send=DMA((2, T, pieces)),
        lat_recv=DMA((T, pieces)),
        ctx_send=DMA((S,)),
        ctx_fsend=DMA((S,)),
        ctx_recv=DMA((2, S)),
        st_send=DMA((2, n)),
        st_recv=DMA((2, n)),
        p1_send=DMA((NC, X)),
        p1_recv=DMA((NC, X)),
        p2_send=DMA((NC,)),
        p2_recv=DMA((NC,)),
        x_send=DMA((NC, X)),
        x_recv=DMA((NC, X)),
    )
    VMEM = pl.BlockSpec(memory_space=pltpu.VMEM)
    ANY = pl.BlockSpec(memory_space=pl.ANY)
    return pl.pallas_call(
        functools.partial(kernel, S, T, tuple(scratch)),
        out_shape=jax.ShapeDtypeStruct((R, D), BF16),
        in_specs=[ANY] * 15,
        out_specs=VMEM,
        scratch_shapes=list(scratch.values()),
        compiler_params=pltpu.CompilerParams(
            collective_id=0, has_side_effects=True, vmem_limit_bytes=60 * 1024 * 1024
        ),
    )(
        latent,
        cond.reshape(Mr // 128, 128),
        context_cond.reshape(Mr // 128, 128),
        context,
        norm_gain.reshape(GD, 128),
        mod_shift,
        mod_scale,
        mod_gate,
        w_query,
        w_key,
        w_value,
        w_gate,
        w_out,
        decay_rate,
        context_gain,
    )


def solution(mesh):
    return jax.shard_map(
        functools.partial(body, mesh.shape["sp"], mesh.shape["tp"]),
        mesh=mesh,
        in_specs=(
            P(("grp", "sp", "tp"), None),
            P(("grp", "sp")),
            P(("grp", "sp"), None),
            P("sp"),
            P(),
            P("sp", "tp"),
            P("sp", "tp"),
            P("sp", "tp"),
            P(None, "tp"),
            P(None, "tp"),
            P(None, "tp"),
            P(None, "tp"),
            P("tp", None),
            P(None, "tp"),
            P("tp"),
        ),
        out_specs=P(("grp", "sp", "tp"), None),
        check_vma=False,
    )
```

```python
import functools
import math
from types import SimpleNamespace

import jax
import jax.numpy as jnp
from jax import lax
from jax.experimental import pallas as pl
from jax.experimental.pallas import tpu as pltpu
from jax.sharding import PartitionSpec as P

DK = 256
GRID_W = 128
TILE = 256
PIECE = 16
EARLY = 1
OWN = 1
CHUNK = 32
LAG = (5, 5)
PRE = 3
NC = 4
norm_eps = 1e-06
rope_base = 10000.0
MESH = pl.DeviceIdType.MESH
F32, BF16 = jnp.float32, jnp.bfloat16


def dot(a, b):
    return jnp.dot(a, b, preferred_element_type=F32)


def dot_tn(a, b):
    return lax.dot_general(a, b, (((0,), (0,)), ((), ())), preferred_element_type=F32)


def dot_nt(a, b):
    return lax.dot_general(a, b, (((1,), (1,)), ((), ())), preferred_element_type=F32)


def remote(src, dst, send, recv, where):
    return pltpu.make_async_remote_copy(
        src_ref=src, dst_ref=dst, send_sem=send, recv_sem=recv, device_id=where, device_id_type=MESH
    )


def rows_of(start, size):
    return pl.ds(pl.multiple_of(start, size), size)


def cols(j, size):
    return pl.ds(pl.multiple_of(j * size, size), size)


def drain(ref, sem):
    pltpu.make_async_copy(ref, ref, sem).wait()


def tiled(x, count):
    return jnp.concatenate([x] * count, axis=0) if count > 1 else x


def kernel(S, T, names, *refs):
    (
        latent,
        cond,
        context_cond,
        context,
        norm_gain,
        mod_shift,
        mod_scale,
        mod_gate,
        w_query,
        w_key,
        w_value,
        w_gate,
        w_out,
        decay_in,
        gain_in,
        out,
    ) = refs[:16]
    r = SimpleNamespace(**dict(zip(names, refs[16:])))

    sp, tp = lax.axis_index("sp"), lax.axis_index("tp")
    R, D = latent.shape
    Cr = context.shape[0]
    half = Cr // 2
    CT = Cr * S
    span = R * T
    nh = w_query.shape[1] // DK
    DV = w_value.shape[1] // nh
    Mr, Mc = mod_shift.shape
    G, GD = Mc // 128, D // 128
    X = T // 2
    pieces = R // PIECE
    chip, core = tp // 2, lax.rem(tp, 2)
    partner = tp + 1 - 2 * core
    is_end = jnp.logical_or(sp == 0, sp == S - 1)
    W = D // NC
    per_head = DK // CHUNK
    n = nh * per_head
    hop = (sp, S - 1 - sp)
    after = (sp + 1, sp - 1)
    before = (sp - 1, sp + 1)
    sp_peers = [lax.rem(sp + k, S) for k in range(1, S)]
    others = [lax.rem(chip + k, X) for k in range(1, X)]
    origins = [lax.rem(chip + X - k, X) for k in range(1, X)]
    peers = [
        (lax.rem(sp + i, S), lax.rem(tp + j, T)) for i in range(S) for j in range(T) if i or j
    ]

    barrier = pltpu.get_barrier_semaphore()
    for a, b in peers:
        pl.semaphore_signal(
            barrier, inc=1, device_id={"sp": a, "tp": b}, device_id_type=MESH
        )

    own = rows_of(tp * R, R)
    pairs = [
        (latent, r.x_all.at[own]),
        (cond, r.cond),
        (context_cond, r.ccond),
        (mod_shift, r.m_shift),
        (mod_scale, r.m_scale),
        (mod_gate, r.m_gate),
        (decay_in, r.decay),
        (gain_in, r.gain),
        (norm_gain, r.ngain),
        (context, r.c_all.at[rows_of(sp * Cr, Cr)]),
        (w_key, r.vk),
        (w_value, r.vv),
        (w_query, r.vq),
        (w_gate, r.vg),
        (w_out, r.vo),
    ]
    loads = [
        pltpu.make_async_copy(src, dst, r.load_sem.at[i]) for i, (src, dst) in enumerate(pairs)
    ]
    for copy in loads:
        copy.start()

    def lat_copy(owner, p, to, sem):
        place = rows_of(owner * R + p * PIECE, PIECE)
        return remote(r.x_all.at[place], r.x_all.at[place], r.lat_send.at[0], sem, {"tp": to})

    def lat_whole(owner, to, sem):
        place = rows_of(owner * R, R)
        return remote(r.x_all.at[place], r.x_all.at[place], r.lat_send.at[0], sem, {"tp": to})

    def lat_pieces(begin, end):
        for p in range(begin, end):
            for k, o in enumerate(others):
                lat_copy(tp, p, 2 * o + core, r.lat_recv.at[k, p]).start()

    def greet():
        loads[0].wait()
        pl.semaphore_wait(barrier, len(peers))
        lat_pieces(0, EARLY)

    late = 2 * sp >= S
    pl.when(late)(greet)

    for copy in loads[1:3]:
        copy.wait()

    def silu_row(ref):
        v = ref[...].astype(F32)
        v = v / (1.0 + jnp.exp(-v))
        return jnp.concatenate([v[g : g + 1, :] for g in range(Mr // 128)], axis=1)

    rows = jnp.concatenate(
        [silu_row(r.cond), silu_row(r.ccond), jnp.zeros((14, Mr), F32)], axis=0
    ).astype(BF16)
    loads[3].wait()
    shift_part = dot(rows, r.m_shift[...])
    loads[4].wait()
    scale_part = dot(rows, r.m_scale[...])

    me = sp * T + tp

    def lanes(x, row, g):
        return x[row : row + 1, g * 128 : (g + 1) * 128]

    for g in range(G):
        r.m1[me, g : g + 1, :] = lanes(shift_part, 0, g)
        r.m1[me, G + g : G + g + 1, :] = lanes(scale_part, 0, g)

    def m_copy(ref, i, to):
        return remote(
            ref.at[me], ref.at[me], r.m_send.at[i], r.m_recv.at[i], {"sp": to[0], "tp": to[1]}
        )

    def ctx_copy(owner, part_core, recv, where):
        place = rows_of(owner * Cr + part_core * half, half)
        return remote(r.c_all.at[place], r.c_all.at[place], r.ctx_send.at[0], recv, where)

    pl.when(jnp.logical_not(late))(greet)

    for to in peers:
        m_copy(r.m1, 0, to).start()
    lat_pieces(EARLY, pieces)
    lat_whole(tp, partner, r.lat_part.at[0]).start()

    loads[5].wait()
    gate_part = dot(rows, r.m_gate[...])
    for g in range(G):
        r.m2[me, g : g + 1, :] = lanes(shift_part, 1, g)
        r.m2[me, G + g : G + g + 1, :] = lanes(scale_part, 1, g)
        r.m2[me, 2 * G + g : 2 * G + g + 1, :] = lanes(gate_part, 0, g)
    loads[9].wait()
    for to in peers:
        m_copy(r.m2, 1, to).start()
    for to in sp_peers:
        ctx_copy(sp, core, r.ctx_recv.at[0], {"sp": to}).start()

    F = DK // 4
    pos = (lax.broadcasted_iota(jnp.int32, (span, 2 * F), 0) + sp * span).astype(F32)
    lane = lax.broadcasted_iota(jnp.int32, (span, 2 * F), 1)
    grid_row = jnp.floor(pos * (1.0 / GRID_W))
    grid_col = pos - grid_row * GRID_W
    freq = jnp.where(lane < F, lane, lane - F).astype(F32)
    angle = jnp.where(lane < F, grid_row, grid_col) * jnp.exp(freq * (-math.log(rope_base) / F))
    r.cos_t[...] = jnp.cos(angle)
    r.sin_t[...] = jnp.sin(angle)

    for copy in loads[6:9]:
        copy.wait()

    def decay_tables(h, _):
        a, b = r.decay[0, h], r.decay[1, h]
        place = lax.broadcasted_iota(jnp.int32, (span, 128), 0).astype(F32)
        r.ktab[0, h] = jnp.exp(-a * (span - 1.0 - place))
        r.ktab[1, h] = jnp.exp(-b * place)
        r.qtab[0, h] = jnp.exp(-a * (place + 1.0))
        r.qtab[1, h] = jnp.exp(-b * (span - place))
        far = lax.broadcasted_iota(jnp.int32, (CT, 128), 0).astype(F32)
        r.ctab[0, h] = jnp.exp(-a * (CT - 1.0 - far))
        r.ctab[1, h] = jnp.exp(-b * far)
        for d, rate in enumerate((a, b)):
            r.fade[d, h] = jnp.exp(jnp.full((8, DV), -rate * span, F32))
        gap = (
            lax.broadcasted_iota(jnp.int32, (span, span), 0)
            - lax.broadcasted_iota(jnp.int32, (span, span), 1)
        ).astype(F32)
        mask = jnp.where(gap >= 0, jnp.exp(-a * jnp.maximum(gap, 0.0)), 0.0)
        mask += jnp.where(gap <= 0, jnp.exp(-b * jnp.maximum(-gap, 0.0)), 0.0)
        r.mask[h] = mask
        return 0

    lax.fori_loop(0, nh, decay_tables, 0)

    def stat(src, dst, start, count):
        place = rows_of(start, count)
        x = src[place, :].astype(F32)
        inv = lax.rsqrt(jnp.mean(x * x, axis=-1, keepdims=True) + norm_eps)
        dst[place, :] = jnp.broadcast_to(inv, (count, 128))

    def apply(src, dst, inv, start, count, row):
        place = rows_of(start, count)
        scale = inv[place, :]
        for j in range(GD):
            c = slice(j * 128, (j + 1) * 128)
            mult = tiled(r.mult[row, :, c], count // 8)
            shift = tiled(r.shift[row, :, c], count // 8)
            dst[place, c] = (src[place, c].astype(F32) * scale * mult + shift).astype(BF16)

    def spread(row, source, at_shift, at_scale):
        for t in range(T):
            total = source[t]
            for s in range(1, S):
                total = total + source[s * T + t]
            r.g16[0, t * G : (t + 1) * G, :] = total[at_shift : at_shift + G]
            r.g16[1, t * G : (t + 1) * G, :] = total[at_scale : at_scale + G]
            if row:
                r.g16[2, t * G : (t + 1) * G, :] = total[2 * G : 3 * G]
        r.g16[1] = r.ngain[...].astype(F32) * (1.0 + r.g16[1])
        for j in range(GD):
            c = slice(j * 128, (j + 1) * 128)
            r.shift[row, :, c] = jnp.broadcast_to(r.g16[0, j : j + 1, :], (8, 128))
            r.mult[row, :, c] = jnp.broadcast_to(r.g16[1, j : j + 1, :], (8, 128))
            if row:
                r.gate[:, c] = jnp.broadcast_to(r.g16[2, j : j + 1, :], (8, 128))

    def pass_on(p):
        for k, o in enumerate(origins):
            owner = 2 * o + core
            lat_copy(owner, p, tp, r.lat_recv.at[k, p]).wait_recv()
            lat_copy(owner, p, partner, r.lat_fwd.at[k]).start()

    def rows_done(owner):
        stat(r.x_all, r.inv, owner * R, R)
        apply(r.x_all, r.h, r.inv, owner * R, R, 0)

    scale_k = DK**-0.5

    def rotated(x, place):
        u, w = x[:, : DK // 2], x[:, DK // 2 :]
        c, s = r.cos_t[place, :], r.sin_t[place, :]
        return jnp.concatenate([u * c - w * s, w * c + u * s], axis=1).astype(BF16)

    def st_copy(d, c, to):
        place = rows_of(c * CHUNK, CHUNK)
        return remote(
            r.st_out.at[d, place],
            r.st_in.at[d, place],
            r.st_send.at[d],
            r.st_recv.at[d, c],
            {"sp": to},
        )

    first = jnp.where(2 * sp < S, 0, 1)
    onward = jnp.where(2 * sp < S, sp + 1, sp - 1)

    def wide(x):
        return jnp.concatenate([x] * (DK // 128), axis=1)

    def key_value(h, o):
        place = rows_of(2 * o * R, 2 * R)
        hidden = r.h[place, :]
        keys = dot(hidden, r.vk[:, cols(h, DK)]) * scale_k
        r.k[h, place, :] = rotated(keys, place)
        r.v[place, cols(h, DV)] = dot(hidden, r.vv[:, cols(h, DV)]).astype(BF16)

    def local_state(h, d):
        keys = (r.k[h].astype(F32) * wide(r.ktab[d, h])).astype(BF16)
        r.loc[d, cols(h, DK), :] = dot_tn(keys, r.v[:, cols(h, DV)])

    def own_rows(h, _):
        key_value(h, chip)
        return 0

    def head_states(h, _):
        for o in others:
            key_value(h, o)
        local_state(h, first)

        @pl.when(is_end)
        def _():
            for c in range(per_head):
                place = rows_of(h * DK + c * CHUNK, CHUNK)
                r.st_out[first, place, :] = r.loc[first, place, :].astype(BF16)
                st_copy(first, h * per_head + c, onward).start()

        local_state(h, 1 - first)
        return 0

    stat(r.x_all, r.inv, tp * R, R)
    for p in range(pieces - 2):
        pass_on(p)
    drain(r.m1.at[pl.ds(0, len(peers))], r.m_recv.at[0])
    spread(0, r.m1, 0, G)
    apply(r.x_all, r.h, r.inv, tp * R, R, 0)
    lat_whole(partner, partner, r.lat_part.at[0]).wait_recv()
    rows_done(partner)
    loads[10].wait()
    loads[11].wait()
    for p in range(max(pieces - 2, 0), pieces - 1):
        pass_on(p)
    lax.fori_loop(0, min(nh, OWN), own_rows, 0)
    pass_on(pieces - 1)
    for o in origins:
        rows_done(2 * o + core)
    lax.fori_loop(min(nh, OWN), nh, own_rows, 0)
    for k, o in enumerate(origins):
        owner = 2 * o + 1 - core
        lat_whole(owner, owner, r.lat_fwd.at[k]).wait_recv()
        rows_done(owner)
    lax.fori_loop(0, nh, head_states, 0)

    def relay(d, c):
        st_copy(d, c, before[d]).wait_recv()
        place = rows_of(c * CHUNK, CHUNK)
        fade = r.fade[d, lax.div(c, per_head), 0:1, :]
        r.st_out[d, place, :] = (
            r.st_in[d, place, :].astype(F32) * fade + r.loc[d, place, :]
        ).astype(BF16)
        st_copy(d, c, after[d]).start()

    loads[12].wait()
    q_all = dot(r.h[...], r.vq[...])
    for h in range(nh):
        q = rotated(q_all[:, h * DK : (h + 1) * DK], slice(0, span))
        r.q[h] = q
        qf = q.astype(F32)
        r.qab[h, :, :DK] = (qf * wide(r.qtab[0, h])).astype(BF16)
        r.qab[h, :, DK:] = (qf * wide(r.qtab[1, h])).astype(BF16)
    loads[13].wait()
    loads[14].wait()

    def gate_item(j):
        pre = dot(r.h[...], r.vg[:, cols(j, TILE)])
        r.g[:, cols(j, TILE)] = pre / (1.0 + jnp.exp(-pre))

    def within_item(h):
        weights = (dot_nt(r.q[h], r.k[h]) * r.mask[h]).astype(BF16)
        r.ret[h] = dot(weights, r.v[:, cols(h, DV)])

    def ctx_forward_item(_):
        drain(r.c_all.at[rows_of(0, (S - 1) * half)], r.ctx_recv.at[0])
        for p in sp_peers:
            ctx_copy(p, core, r.ctx_recv.at[1], {"tp": partner}).start()
        drain(r.m2.at[pl.ds(0, len(peers))], r.m_recv.at[1])
        spread(1, r.m2, 0, G)

    def ctx_arrive_item(_):
        drain(r.c_all.at[rows_of(0, (S - 1) * half)], r.ctx_recv.at[1])

    def ctx_norm_item(j):
        stat(r.c_all, r.cinv, j * 64, 64)
        apply(r.c_all, r.hc, r.cinv, j * 64, 64, 1)

    M = min(CT, TILE)

    def ctx_key_item(j):
        place, h = rows_of(lax.div(j, nh) * M, M), lax.rem(j, nh)
        r.ck[h, place, :] = (dot(r.hc[place, :], r.vk[:, cols(h, DK)]) * scale_k).astype(BF16)

    nv = nh * DV // TILE

    def ctx_value_item(j):
        place, t = rows_of(lax.div(j, nv) * M, M), lax.rem(j, nv)
        r.cv[place, cols(t, TILE)] = dot(r.hc[place, :], r.vv[:, cols(t, TILE)]).astype(BF16)

    def ctx_state_item(j):
        h, d = lax.div(j, 2), lax.rem(j, 2)
        keys = (r.ck[h].astype(F32) * wide(r.ctab[d, h])).astype(BF16)
        away = jnp.where(d == 0, hop[0], hop[1]).astype(F32) * span
        weight = jnp.exp(jnp.full((1, DV), -r.decay[d, h] * away, F32)) * r.gain[h]
        r.base[d, cols(h, DK), :] = dot_tn(keys, r.cv[:, cols(h, DV)]) * weight

    items = [
        (nv, gate_item),
        (1, ctx_forward_item),
        (nh, within_item),
        (1, ctx_arrive_item),
        (CT // 64, ctx_norm_item),
        (CT // M * nh, ctx_key_item),
        (CT // M * nv, ctx_value_item),
        (2 * nh, ctx_state_item),
    ]
    total_items = sum(count for count, _ in items)
    inner = jnp.logical_not(is_end)

    def lap(i, _):
        for d in (1, 0):
            c = i - PRE - LAG[d] * (hop[d] - 1)

            @pl.when(jnp.logical_and(inner, jnp.logical_and(c >= 0, c < n)))
            def _():
                relay(d, c)

        start = 0
        for count, run in items:

            @pl.when(jnp.logical_and(i >= start, i < start + count))
            def _():
                run(i - start)

            start += count
        return 0

    lax.fori_loop(0, max(PRE + n + max(LAG) * max(S - 3, 0), total_items), lap, 0)

    def project(h, start, count, c):
        return dot(r.gated[h, rows_of(start, count), :], r.vo[h * DV : (h + 1) * DV, cols(c, W)])

    for h in range(nh):
        for d in range(2):

            @pl.when(hop[d] == 0)
            def _():
                r.ent[h, d * DK : (d + 1) * DK, :] = r.base[d, h * DK : (h + 1) * DK, :].astype(
                    BF16
                )

            @pl.when(hop[d] > 0)
            def _():
                def enter(c, _):
                    @pl.when(hop[d] == S - 1)
                    def _():
                        st_copy(d, h * per_head + c, before[d]).wait_recv()

                    place = rows_of(h * DK + c * CHUNK, CHUNK)
                    r.ent[h, rows_of(d * DK + c * CHUNK, CHUNK), :] = (
                        r.st_in[d, place, :].astype(F32) + r.base[d, place, :]
                    ).astype(BF16)
                    return 0

                lax.fori_loop(0, per_head, enter, 0)

        ret = r.ret[h] + dot(r.qab[h], r.ent[h])
        ret = ret - jnp.mean(ret, axis=-1, keepdims=True)
        ret = ret * lax.rsqrt(jnp.mean(ret * ret, axis=-1, keepdims=True) + norm_eps)
        r.gated[h] = (r.g[:, h * DV : (h + 1) * DV] * ret).astype(BF16)
        if h < nh - 1:

            def gather(c, _):
                value = project(h, 0, span, c)
                if h:
                    value = value + r.acc[:, cols(c, W)]
                r.acc[:, cols(c, W)] = value
                return 0

            lax.fori_loop(0, NC, gather, 0)

    def chip_rows(c, o):
        value = project(nh - 1, 2 * o * R, 2 * R, c)
        if nh > 1:
            value = value + r.acc[rows_of(2 * o * R, 2 * R), cols(c, W)]
        value = value.astype(BF16)
        r.part[c, 2 * o] = value[:R]
        r.part[c, 2 * o + 1] = value[R:]

    def p1_copy(c, k, o):
        return remote(
            r.part.at[c, 2 * o + 1 - core],
            r.p1.at[c, k],
            r.out_send.at[0],
            r.p1_recv.at[c, k],
            {"tp": partner},
        )

    def p2_copy(c):
        return remote(
            r.part.at[c, partner], r.p2.at[c], r.out_send.at[0], r.p2_recv.at[0], {"tp": partner}
        )

    def x_copy(c, k, o):
        return remote(
            r.xs.at[c, k],
            r.xr.at[c, k],
            r.out_send.at[0],
            r.x_recv.at[c, k],
            {"tp": 2 * o + core},
        )

    def away(c, _):
        for k, o in enumerate(others):
            chip_rows(c, o)
            p1_copy(c, k, o).start()
        return 0

    lax.fori_loop(0, NC, away, 0)

    def across(c, _):
        for k, o in enumerate(others):
            p1_copy(c, k, o).wait_recv()
            mine = r.part[c, 2 * o + core].astype(F32)
            r.xs[c, k] = (mine + r.p1[c, k].astype(F32)).astype(BF16)
            x_copy(c, k, o).start()
        chip_rows(c, chip)
        p2_copy(c).start()
        return 0

    lax.fori_loop(0, NC, across, 0)

    drain(r.m1.at[pl.ds(0, len(peers))], r.m_send.at[0])
    drain(r.m2.at[pl.ds(0, len(peers))], r.m_send.at[1])
    drain(r.x_all.at[rows_of(0, (T - 1) * R)], r.lat_send.at[0])
    drain(r.c_all.at[rows_of(0, (S - 1) * Cr)], r.ctx_send.at[0])
    for d in range(2):

        @pl.when(hop[d] < S - 1)
        def _():
            drain(r.st_out.at[d], r.st_send.at[d])

    drain(r.p2, r.p2_recv.at[0])

    def final(c, _):
        total = r.part[c, tp].astype(F32) + r.p2[c].astype(F32)
        for k, o in enumerate(origins):
            x_copy(c, k, o).wait_recv()
            total = total + r.xr[c, k].astype(F32)
        mine = r.x_all[own, cols(c, W)].astype(F32)
        gate = tiled(r.gate[:, cols(c, W)], R // 8)
        out[:, cols(c, W)] = (mine + gate * total).astype(BF16)
        return 0

    lax.fori_loop(0, NC, final, 0)
    drain(r.part.at[:, pl.ds(0, T - 1)], r.out_send.at[0])


def body(
    S,
    T,
    latent,
    cond,
    context,
    context_cond,
    norm_gain,
    mod_shift,
    mod_scale,
    mod_gate,
    w_query,
    w_key,
    w_value,
    w_gate,
    w_out,
    decay_rate,
    context_gain,
):
    R, D = latent.shape
    Cr = context.shape[0]
    span, CT = R * T, Cr * S
    nh = w_query.shape[1] // DK
    DV = w_value.shape[1] // nh
    Mr, Mc = mod_shift.shape
    G, GD = Mc // 128, D // 128
    X = T // 2
    W = D // NC
    n = nh * DK // CHUNK
    pieces = R // PIECE
    v = pltpu.VMEM
    DMA = pltpu.SemaphoreType.DMA
    scratch = dict(
        x_all=v((span, D), BF16),
        c_all=v((CT, D), BF16),
        h=v((span, D), BF16),
        hc=v((CT, D), BF16),
        cond=v((Mr // 128, 128), BF16),
        ccond=v((Mr // 128, 128), BF16),
        ngain=v((GD, 128), BF16),
        decay=pltpu.SMEM(decay_rate.shape, F32),
        gain=pltpu.SMEM(context_gain.shape, F32),
        m_shift=v((Mr, Mc), BF16),
        m_scale=v((Mr, Mc), BF16),
        m_gate=v((Mr, Mc), BF16),
        vq=v(w_query.shape, BF16),
        vk=v(w_key.shape, BF16),
        vv=v(w_value.shape, BF16),
        vg=v(w_gate.shape, BF16),
        vo=v(w_out.shape, BF16),
        m1=v((S * T, 2 * G, 128), F32),
        m2=v((S * T, 3 * G, 128), F32),
        g16=v((3, GD, 128), F32),
        shift=v((2, 8, D), F32),
        mult=v((2, 8, D), F32),
        gate=v((8, D), F32),
        inv=v((span, 128), F32),
        cinv=v((CT, 128), F32),
        cos_t=v((span, DK // 2), F32),
        sin_t=v((span, DK // 2), F32),
        ktab=v((2, nh, span, 128), F32),
        qtab=v((2, nh, span, 128), F32),
        ctab=v((2, nh, CT, 128), F32),
        fade=v((2, nh, 8, DV), F32),
        mask=v((nh, span, span), F32),
        q=v((nh, span, DK), BF16),
        qab=v((nh, span, 2 * DK), BF16),
        k=v((nh, span, DK), BF16),
        v=v((span, nh * DV), BF16),
        ck=v((nh, CT, DK), BF16),
        cv=v((CT, nh * DV), BF16),
        g=v((span, nh * DV), F32),
        ret=v((nh, span, DV), F32),
        gated=v((nh, span, DV), BF16),
        loc=v((2, nh * DK, DV), F32),
        base=v((2, nh * DK, DV), F32),
        st_in=v((2, nh * DK, DV), BF16),
        st_out=v((2, nh * DK, DV), BF16),
        ent=v((nh, 2 * DK, DV), BF16),
        acc=v((span, D), F32),
        part=v((NC, T, R, W), BF16),
        p1=v((NC, X - 1, R, W), BF16),
        p2=v((NC, R, W), BF16),
        xs=v((NC, X - 1, R, W), BF16),
        xr=v((NC, X - 1, R, W), BF16),
        load_sem=DMA((15,)),
        m_send=DMA((2,)),
        m_recv=DMA((2,)),
        lat_send=DMA((1,)),
        lat_recv=DMA((X - 1, pieces)),
        lat_part=DMA((1,)),
        lat_fwd=DMA((X - 1,)),
        ctx_send=DMA((1,)),
        ctx_recv=DMA((2,)),
        st_send=DMA((2,)),
        st_recv=DMA((2, n)),
        out_send=DMA((1,)),
        p1_recv=DMA((NC, X - 1)),
        p2_recv=DMA((1,)),
        x_recv=DMA((NC, X - 1)),
    )
    VMEM = pl.BlockSpec(memory_space=pltpu.VMEM)
    ANY = pl.BlockSpec(memory_space=pl.ANY)
    return pl.pallas_call(
        functools.partial(kernel, S, T, tuple(scratch)),
        out_shape=pltpu.VMEM((R, D), BF16),
        in_specs=[ANY] * 15,
        out_specs=VMEM,
        scratch_shapes=list(scratch.values()),
        compiler_params=pltpu.CompilerParams(
            collective_id=0, has_side_effects=True, vmem_limit_bytes=60 * 1024 * 1024
        ),
    )(
        latent,
        cond.reshape(Mr // 128, 128),
        context_cond.reshape(Mr // 128, 128),
        context,
        norm_gain.reshape(GD, 128),
        mod_shift,
        mod_scale,
        mod_gate,
        w_query,
        w_key,
        w_value,
        w_gate,
        w_out,
        decay_rate,
        context_gain,
    )


def solution(mesh):
    return jax.shard_map(
        functools.partial(body, mesh.shape["sp"], mesh.shape["tp"]),
        mesh=mesh,
        in_specs=(
            P(("grp", "sp", "tp"), None),
            P(("grp", "sp")),
            P(("grp", "sp"), None),
            P("sp"),
            P(),
            P("sp", "tp"),
            P("sp", "tp"),
            P("sp", "tp"),
            P(None, "tp"),
            P(None, "tp"),
            P(None, "tp"),
            P(None, "tp"),
            P("tp", None),
            P(None, "tp"),
            P("tp"),
        ),
        out_specs=P(("grp", "sp", "tp"), None),
        check_vma=False,
    )
```

```python
import functools
import math
from types import SimpleNamespace

import jax
import jax.numpy as jnp
from jax import lax
from jax.experimental import pallas as pl
from jax.experimental.pallas import tpu as pltpu
from jax.sharding import PartitionSpec as P

DK = 256
GRID_W = 128
TILE = 256
PIECE = 16
EARLY = 1
OWN = 1
CHUNK = 32
LAG = (6, 4)
PRE = 1
SPARE = (1, 1)
NC = 2
norm_eps = 1e-06
rope_base = 10000.0
MESH = pl.DeviceIdType.MESH
F32, BF16 = jnp.float32, jnp.bfloat16


def dot(a, b):
    return jnp.dot(a, b, preferred_element_type=F32)


def dot_tn(a, b):
    return lax.dot_general(a, b, (((0,), (0,)), ((), ())), preferred_element_type=F32)


def dot_nt(a, b):
    return lax.dot_general(a, b, (((1,), (1,)), ((), ())), preferred_element_type=F32)


def remote(src, dst, send, recv, where):
    return pltpu.make_async_remote_copy(
        src_ref=src, dst_ref=dst, send_sem=send, recv_sem=recv, device_id=where, device_id_type=MESH
    )


def rows_of(start, size):
    return pl.ds(pl.multiple_of(start, size), size)


def cols(j, size):
    return pl.ds(pl.multiple_of(j * size, size), size)


def drain(ref, sem):
    pltpu.make_async_copy(ref, ref, sem).wait()


def tiled(x, count):
    return jnp.concatenate([x] * count, axis=0) if count > 1 else x


def kernel(S, T, names, *refs):
    (
        latent,
        cond,
        context_cond,
        context,
        norm_gain,
        mod_shift,
        mod_scale,
        mod_gate,
        w_query,
        w_key,
        w_value,
        w_gate,
        w_out,
        decay_in,
        gain_in,
        out,
    ) = refs[:16]
    r = SimpleNamespace(**dict(zip(names, refs[16:])))

    sp, tp = lax.axis_index("sp"), lax.axis_index("tp")
    R, D = latent.shape
    Cr = context.shape[0]
    half = Cr // 2
    CT = Cr * S
    span = R * T
    nh = w_query.shape[1] // DK
    DV = w_value.shape[1] // nh
    Mr, Mc = mod_shift.shape
    G, GD = Mc // 128, D // 128
    X = T // 2
    pieces = R // PIECE
    chip, core = tp // 2, lax.rem(tp, 2)
    partner = tp + 1 - 2 * core
    is_end = jnp.logical_or(sp == 0, sp == S - 1)
    W = D // NC
    per_head = DK // CHUNK
    n = nh * per_head
    hop = (sp, S - 1 - sp)
    after = (sp + 1, sp - 1)
    before = (sp - 1, sp + 1)
    sp_peers = [lax.rem(sp + k, S) for k in range(1, S)]
    others = [lax.rem(chip + k, X) for k in range(1, X)]
    origins = [lax.rem(chip + X - k, X) for k in range(1, X)]
    peers = [
        (lax.rem(sp + i, S), lax.rem(tp + j, T)) for i in range(S) for j in range(T) if i or j
    ]

    barrier = pltpu.get_barrier_semaphore()
    for a, b in peers:
        pl.semaphore_signal(
            barrier, inc=1, device_id={"sp": a, "tp": b}, device_id_type=MESH
        )

    own = rows_of(tp * R, R)
    pairs = [
        (latent, r.x_all.at[own]),
        (cond, r.cond),
        (context_cond, r.ccond),
        (mod_shift, r.m_shift),
        (mod_scale, r.m_scale),
        (mod_gate, r.m_gate),
        (decay_in, r.decay),
        (gain_in, r.gain),
        (norm_gain, r.ngain),
        (context, r.c_all.at[rows_of(sp * Cr, Cr)]),
        (w_key, r.vk),
        (w_value, r.vv),
        (w_query, r.vq),
        (w_gate, r.vg),
        (w_out, r.vo),
    ]
    loads = [
        pltpu.make_async_copy(src, dst, r.load_sem.at[i]) for i, (src, dst) in enumerate(pairs)
    ]
    for copy in loads:
        copy.start()

    def lat_copy(owner, p, to, sem):
        place = rows_of(owner * R + p * PIECE, PIECE)
        return remote(r.x_all.at[place], r.x_all.at[place], r.lat_send.at[0], sem, {"tp": to})

    def lat_whole(owner, to, sem):
        place = rows_of(owner * R, R)
        return remote(r.x_all.at[place], r.x_all.at[place], r.lat_send.at[0], sem, {"tp": to})

    def lat_pieces(begin, end):
        for p in range(begin, end):
            for k, o in enumerate(others):
                lat_copy(tp, p, 2 * o + core, r.lat_recv.at[k, p]).start()

    def greet():
        loads[0].wait()
        pl.semaphore_wait(barrier, len(peers))
        lat_pieces(0, EARLY)

    late = 2 * sp >= S
    pl.when(late)(greet)

    for copy in loads[1:3]:
        copy.wait()

    def silu_row(ref):
        v = ref[...].astype(F32)
        v = v / (1.0 + jnp.exp(-v))
        return jnp.concatenate([v[g : g + 1, :] for g in range(Mr // 128)], axis=1)

    rows = jnp.concatenate(
        [silu_row(r.cond), silu_row(r.ccond), jnp.zeros((14, Mr), F32)], axis=0
    ).astype(BF16)
    loads[3].wait()
    shift_part = dot(rows, r.m_shift[...])
    loads[4].wait()
    scale_part = dot(rows, r.m_scale[...])

    me = sp * T + tp

    def lanes(x, row, g):
        return x[row : row + 1, g * 128 : (g + 1) * 128]

    for g in range(G):
        r.m1[me, g : g + 1, :] = lanes(shift_part, 0, g)
        r.m1[me, G + g : G + g + 1, :] = lanes(scale_part, 0, g)

    def m_copy(ref, i, to):
        return remote(
            ref.at[me], ref.at[me], r.m_send.at[i], r.m_recv.at[i], {"sp": to[0], "tp": to[1]}
        )

    def ctx_copy(owner, part_core, recv, where):
        place = rows_of(owner * Cr + part_core * half, half)
        return remote(r.c_all.at[place], r.c_all.at[place], r.ctx_send.at[0], recv, where)

    pl.when(jnp.logical_not(late))(greet)

    for to in peers:
        m_copy(r.m1, 0, to).start()
    lat_pieces(EARLY, pieces)
    lat_whole(tp, partner, r.lat_part.at[0]).start()

    loads[5].wait()
    gate_part = dot(rows, r.m_gate[...])
    for g in range(G):
        r.m2[me, g : g + 1, :] = lanes(shift_part, 1, g)
        r.m2[me, G + g : G + g + 1, :] = lanes(scale_part, 1, g)
        r.m2[me, 2 * G + g : 2 * G + g + 1, :] = lanes(gate_part, 0, g)
    loads[9].wait()
    for to in peers:
        m_copy(r.m2, 1, to).start()
    for to in sp_peers:
        ctx_copy(sp, core, r.ctx_recv.at[0], {"sp": to}).start()

    F = DK // 4
    pos = (lax.broadcasted_iota(jnp.int32, (span, 2 * F), 0) + sp * span).astype(F32)
    lane = lax.broadcasted_iota(jnp.int32, (span, 2 * F), 1)
    grid_row = jnp.floor(pos * (1.0 / GRID_W))
    grid_col = pos - grid_row * GRID_W
    freq = jnp.where(lane < F, lane, lane - F).astype(F32)
    angle = jnp.where(lane < F, grid_row, grid_col) * jnp.exp(freq * (-math.log(rope_base) / F))
    r.cos_t[...] = jnp.cos(angle)
    r.sin_t[...] = jnp.sin(angle)

    for copy in loads[6:9]:
        copy.wait()

    def decay_tables(h, _):
        a, b = r.decay[0, h], r.decay[1, h]
        place = lax.broadcasted_iota(jnp.int32, (span, 128), 0).astype(F32)
        r.ktab[0, h] = jnp.exp(-a * (span - 1.0 - place))
        r.ktab[1, h] = jnp.exp(-b * place)
        r.qtab[0, h] = jnp.exp(-a * (place + 1.0))
        r.qtab[1, h] = jnp.exp(-b * (span - place))
        far = lax.broadcasted_iota(jnp.int32, (CT, 128), 0).astype(F32)
        r.ctab[0, h] = jnp.exp(-a * (CT - 1.0 - far))
        r.ctab[1, h] = jnp.exp(-b * far)
        for d, rate in enumerate((a, b)):
            r.fade[d, h] = jnp.exp(jnp.full((8, DV), -rate * span, F32))
        gap = (
            lax.broadcasted_iota(jnp.int32, (span, span), 0)
            - lax.broadcasted_iota(jnp.int32, (span, span), 1)
        ).astype(F32)
        mask = jnp.where(gap >= 0, jnp.exp(-a * jnp.maximum(gap, 0.0)), 0.0)
        mask += jnp.where(gap <= 0, jnp.exp(-b * jnp.maximum(-gap, 0.0)), 0.0)
        r.mask[h] = mask
        return 0

    lax.fori_loop(0, nh, decay_tables, 0)

    def stat(src, dst, start, count):
        place = rows_of(start, count)
        x = src[place, :].astype(F32)
        inv = lax.rsqrt(jnp.mean(x * x, axis=-1, keepdims=True) + norm_eps)
        dst[place, :] = jnp.broadcast_to(inv, (count, 128))

    def apply(src, dst, inv, start, count, row):
        place = rows_of(start, count)
        scale = inv[place, :]
        for j in range(GD):
            c = slice(j * 128, (j + 1) * 128)
            mult = tiled(r.mult[row, :, c], count // 8)
            shift = tiled(r.shift[row, :, c], count // 8)
            dst[place, c] = (src[place, c].astype(F32) * scale * mult + shift).astype(BF16)

    def spread(row, source, at_shift, at_scale):
        for t in range(T):
            total = source[t]
            for s in range(1, S):
                total = total + source[s * T + t]
            r.g16[0, t * G : (t + 1) * G, :] = total[at_shift : at_shift + G]
            r.g16[1, t * G : (t + 1) * G, :] = total[at_scale : at_scale + G]
            if row:
                r.g16[2, t * G : (t + 1) * G, :] = total[2 * G : 3 * G]
        r.g16[1] = r.ngain[...].astype(F32) * (1.0 + r.g16[1])
        for j in range(GD):
            c = slice(j * 128, (j + 1) * 128)
            r.shift[row, :, c] = jnp.broadcast_to(r.g16[0, j : j + 1, :], (8, 128))
            r.mult[row, :, c] = jnp.broadcast_to(r.g16[1, j : j + 1, :], (8, 128))
            if row:
                r.gate[:, c] = jnp.broadcast_to(r.g16[2, j : j + 1, :], (8, 128))

    def pass_on(p):
        for k, o in enumerate(origins):
            owner = 2 * o + core
            lat_copy(owner, p, tp, r.lat_recv.at[k, p]).wait_recv()
            lat_copy(owner, p, partner, r.lat_fwd.at[k]).start()

    def rows_done(owner):
        stat(r.x_all, r.inv, owner * R, R)
        apply(r.x_all, r.h, r.inv, owner * R, R, 0)

    scale_k = DK**-0.5

    def rotated(x, place):
        u, w = x[:, : DK // 2], x[:, DK // 2 :]
        c, s = r.cos_t[place, :], r.sin_t[place, :]
        return jnp.concatenate([u * c - w * s, w * c + u * s], axis=1).astype(BF16)

    def st_copy(d, c, to):
        place = rows_of(c * CHUNK, CHUNK)
        return remote(
            r.st_out.at[d, place],
            r.st_in.at[d, place],
            r.st_send.at[d],
            r.st_recv.at[d, c],
            {"sp": to},
        )

    first = jnp.where(2 * sp < S, 0, 1)
    onward = jnp.where(2 * sp < S, sp + 1, sp - 1)

    def wide(x):
        return jnp.concatenate([x] * (DK // 128), axis=1)

    def key_value(h, o):
        place = rows_of(2 * o * R, 2 * R)
        hidden = r.h[place, :]
        keys = dot(hidden, r.vk[:, cols(h, DK)]) * scale_k
        r.k[h, place, :] = rotated(keys, place)
        r.v[place, cols(h, DV)] = dot(hidden, r.vv[:, cols(h, DV)]).astype(BF16)

    def local_state(h, d):
        keys = (r.k[h].astype(F32) * wide(r.ktab[d, h])).astype(BF16)
        r.loc[d, cols(h, DK), :] = dot_tn(keys, r.v[:, cols(h, DV)])

    def own_rows(h, _):
        key_value(h, chip)
        return 0

    def head_states(h, _):
        for o in others:
            key_value(h, o)
        local_state(h, first)

        @pl.when(is_end)
        def _():
            for c in range(per_head):
                place = rows_of(h * DK + c * CHUNK, CHUNK)
                r.st_out[first, place, :] = r.loc[first, place, :].astype(BF16)
                st_copy(first, h * per_head + c, onward).start()

        local_state(h, 1 - first)
        return 0

    stat(r.x_all, r.inv, tp * R, R)
    for p in range(pieces - 2):
        pass_on(p)
    drain(r.m1.at[pl.ds(0, len(peers))], r.m_recv.at[0])
    spread(0, r.m1, 0, G)
    apply(r.x_all, r.h, r.inv, tp * R, R, 0)
    lat_whole(partner, partner, r.lat_part.at[0]).wait_recv()
    rows_done(partner)
    loads[10].wait()
    loads[11].wait()
    for p in range(max(pieces - 2, 0), pieces - 1):
        pass_on(p)
    lax.fori_loop(0, min(nh, OWN), own_rows, 0)
    pass_on(pieces - 1)
    for o in origins:
        rows_done(2 * o + core)
    lax.fori_loop(min(nh, OWN), nh, own_rows, 0)
    for k, o in enumerate(origins):
        owner = 2 * o + 1 - core
        lat_whole(owner, owner, r.lat_fwd.at[k]).wait_recv()
        rows_done(owner)
    lax.fori_loop(0, nh, head_states, 0)

    def relay(d, c):
        st_copy(d, c, before[d]).wait_recv()
        place = rows_of(c * CHUNK, CHUNK)
        fade = r.fade[d, lax.div(c, per_head), 0:1, :]
        r.st_out[d, place, :] = (
            r.st_in[d, place, :].astype(F32) * fade + r.loc[d, place, :]
        ).astype(BF16)
        st_copy(d, c, after[d]).start()

    loads[12].wait()
    q_all = dot(r.h[...], r.vq[...])
    for h in range(nh):
        q = rotated(q_all[:, h * DK : (h + 1) * DK], slice(0, span))
        r.q[h] = q
        qf = q.astype(F32)
        r.qab[h, :, :DK] = (qf * wide(r.qtab[0, h])).astype(BF16)
        r.qab[h, :, DK:] = (qf * wide(r.qtab[1, h])).astype(BF16)
    loads[13].wait()
    loads[14].wait()

    def gate_item(j):
        pre = dot(r.h[...], r.vg[:, cols(j, TILE)])
        r.g[:, cols(j, TILE)] = pre / (1.0 + jnp.exp(-pre))

    def within_item(h):
        weights = (dot_nt(r.q[h], r.k[h]) * r.mask[h]).astype(BF16)
        r.ret[h] = dot(weights, r.v[:, cols(h, DV)])

    def ctx_forward_item(_):
        drain(r.c_all.at[rows_of(0, (S - 1) * half)], r.ctx_recv.at[0])
        for p in sp_peers:
            ctx_copy(p, core, r.ctx_recv.at[1], {"tp": partner}).start()
        drain(r.m2.at[pl.ds(0, len(peers))], r.m_recv.at[1])
        spread(1, r.m2, 0, G)

    def ctx_arrive_item(_):
        drain(r.c_all.at[rows_of(0, (S - 1) * half)], r.ctx_recv.at[1])

    def ctx_norm_item(j):
        stat(r.c_all, r.cinv, j * 64, 64)
        apply(r.c_all, r.hc, r.cinv, j * 64, 64, 1)

    M = min(CT, TILE)

    def ctx_key_item(j):
        place, h = rows_of(lax.div(j, nh) * M, M), lax.rem(j, nh)
        r.ck[h, place, :] = (dot(r.hc[place, :], r.vk[:, cols(h, DK)]) * scale_k).astype(BF16)

    nv = nh * DV // TILE

    def ctx_value_item(j):
        place, t = rows_of(lax.div(j, nv) * M, M), lax.rem(j, nv)
        r.cv[place, cols(t, TILE)] = dot(r.hc[place, :], r.vv[:, cols(t, TILE)]).astype(BF16)

    def ctx_state_item(j):
        h, d = lax.div(j, 2), lax.rem(j, 2)
        keys = (r.ck[h].astype(F32) * wide(r.ctab[d, h])).astype(BF16)
        away = jnp.where(d == 0, hop[0], hop[1]).astype(F32) * span
        weight = jnp.exp(jnp.full((1, DV), -r.decay[d, h] * away, F32)) * r.gain[h]
        r.base[d, cols(h, DK), :] = dot_tn(keys, r.cv[:, cols(h, DV)]) * weight

    items = [
        (nv, gate_item),
        (nh, within_item),
        (SPARE[0], None),
        (1, ctx_forward_item),
        (SPARE[1], None),
        (1, ctx_arrive_item),
        (CT // 64, ctx_norm_item),
        (CT // M * nh, ctx_key_item),
        (CT // M * nv, ctx_value_item),
        (2 * nh, ctx_state_item),
    ]
    total_items = sum(count for count, _ in items)
    inner = jnp.logical_not(is_end)

    def lap(i, _):
        for d in (1, 0):
            c = i - PRE - LAG[d] * (hop[d] - 1)

            @pl.when(jnp.logical_and(inner, jnp.logical_and(c >= 0, c < n)))
            def _():
                relay(d, c)

        start = 0
        for count, run in items:
            if run is not None:

                @pl.when(jnp.logical_and(i >= start, i < start + count))
                def _():
                    run(i - start)

            start += count
        return 0

    lax.fori_loop(0, max(PRE + n + max(LAG) * max(S - 3, 0), total_items), lap, 0)

    def project(h, start, count, c):
        return dot(r.gated[h, rows_of(start, count), :], r.vo[h * DV : (h + 1) * DV, cols(c, W)])

    for h in range(nh):
        for d in range(2):

            @pl.when(hop[d] == 0)
            def _():
                r.ent[h, d * DK : (d + 1) * DK, :] = r.base[d, h * DK : (h + 1) * DK, :].astype(
                    BF16
                )

            @pl.when(hop[d] > 0)
            def _():
                def enter(c, _):
                    @pl.when(hop[d] == S - 1)
                    def _():
                        st_copy(d, h * per_head + c, before[d]).wait_recv()

                    place = rows_of(h * DK + c * CHUNK, CHUNK)
                    r.ent[h, rows_of(d * DK + c * CHUNK, CHUNK), :] = (
                        r.st_in[d, place, :].astype(F32) + r.base[d, place, :]
                    ).astype(BF16)
                    return 0

                lax.fori_loop(0, per_head, enter, 0)

        ret = r.ret[h] + dot(r.qab[h], r.ent[h])
        ret = ret - jnp.mean(ret, axis=-1, keepdims=True)
        ret = ret * lax.rsqrt(jnp.mean(ret * ret, axis=-1, keepdims=True) + norm_eps)
        r.gated[h] = (r.g[:, h * DV : (h + 1) * DV] * ret).astype(BF16)
        if h < nh - 1:

            def gather(c, _):
                value = project(h, 0, span, c)
                if h:
                    value = value + r.acc[:, cols(c, W)]
                r.acc[:, cols(c, W)] = value
                return 0

            lax.fori_loop(0, NC, gather, 0)

    def chip_rows(c, o):
        value = project(nh - 1, 2 * o * R, 2 * R, c)
        if nh > 1:
            value = value + r.acc[rows_of(2 * o * R, 2 * R), cols(c, W)]
        value = value.astype(BF16)
        r.part[c, 2 * o] = value[:R]
        r.part[c, 2 * o + 1] = value[R:]

    def p1_copy(c, k, o):
        return remote(
            r.part.at[c, 2 * o + 1 - core],
            r.p1.at[c, k],
            r.out_send.at[0],
            r.p1_recv.at[c, k],
            {"tp": partner},
        )

    def p2_copy(c):
        return remote(
            r.part.at[c, partner], r.p2.at[c], r.out_send.at[0], r.p2_recv.at[0], {"tp": partner}
        )

    def x_copy(c, k, o):
        return remote(
            r.xs.at[c, k],
            r.xr.at[c, k],
            r.out_send.at[0],
            r.x_recv.at[c, k],
            {"tp": 2 * o + core},
        )

    def away(c, _):
        for k, o in enumerate(others):
            chip_rows(c, o)
            p1_copy(c, k, o).start()
        return 0

    lax.fori_loop(0, NC, away, 0)

    def across(c, _):
        for k, o in enumerate(others):
            p1_copy(c, k, o).wait_recv()
            mine = r.part[c, 2 * o + core].astype(F32)
            r.xs[c, k] = (mine + r.p1[c, k].astype(F32)).astype(BF16)
            x_copy(c, k, o).start()
        chip_rows(c, chip)
        p2_copy(c).start()
        return 0

    lax.fori_loop(0, NC, across, 0)

    drain(r.m1.at[pl.ds(0, len(peers))], r.m_send.at[0])
    drain(r.m2.at[pl.ds(0, len(peers))], r.m_send.at[1])
    drain(r.x_all.at[rows_of(0, (T - 1) * R)], r.lat_send.at[0])
    drain(r.c_all.at[rows_of(0, (S - 1) * Cr)], r.ctx_send.at[0])
    for d in range(2):

        @pl.when(hop[d] < S - 1)
        def _():
            drain(r.st_out.at[d], r.st_send.at[d])

    drain(r.p2, r.p2_recv.at[0])

    def final(c, _):
        total = r.part[c, tp].astype(F32) + r.p2[c].astype(F32)
        for k, o in enumerate(origins):
            x_copy(c, k, o).wait_recv()
            total = total + r.xr[c, k].astype(F32)
        mine = r.x_all[own, cols(c, W)].astype(F32)
        gate = tiled(r.gate[:, cols(c, W)], R // 8)
        out[:, cols(c, W)] = (mine + gate * total).astype(BF16)
        return 0

    lax.fori_loop(0, NC, final, 0)
    drain(r.part.at[:, pl.ds(0, T - 1)], r.out_send.at[0])


def body(
    S,
    T,
    latent,
    cond,
    context,
    context_cond,
    norm_gain,
    mod_shift,
    mod_scale,
    mod_gate,
    w_query,
    w_key,
    w_value,
    w_gate,
    w_out,
    decay_rate,
    context_gain,
):
    R, D = latent.shape
    Cr = context.shape[0]
    span, CT = R * T, Cr * S
    nh = w_query.shape[1] // DK
    DV = w_value.shape[1] // nh
    Mr, Mc = mod_shift.shape
    G, GD = Mc // 128, D // 128
    X = T // 2
    W = D // NC
    n = nh * DK // CHUNK
    pieces = R // PIECE
    v = pltpu.VMEM
    DMA = pltpu.SemaphoreType.DMA
    scratch = dict(
        x_all=v((span, D), BF16),
        c_all=v((CT, D), BF16),
        h=v((span, D), BF16),
        hc=v((CT, D), BF16),
        cond=v((Mr // 128, 128), BF16),
        ccond=v((Mr // 128, 128), BF16),
        ngain=v((GD, 128), BF16),
        decay=pltpu.SMEM(decay_rate.shape, F32),
        gain=pltpu.SMEM(context_gain.shape, F32),
        m_shift=v((Mr, Mc), BF16),
        m_scale=v((Mr, Mc), BF16),
        m_gate=v((Mr, Mc), BF16),
        vq=v(w_query.shape, BF16),
        vk=v(w_key.shape, BF16),
        vv=v(w_value.shape, BF16),
        vg=v(w_gate.shape, BF16),
        vo=v(w_out.shape, BF16),
        m1=v((S * T, 2 * G, 128), F32),
        m2=v((S * T, 3 * G, 128), F32),
        g16=v((3, GD, 128), F32),
        shift=v((2, 8, D), F32),
        mult=v((2, 8, D), F32),
        gate=v((8, D), F32),
        inv=v((span, 128), F32),
        cinv=v((CT, 128), F32),
        cos_t=v((span, DK // 2), F32),
        sin_t=v((span, DK // 2), F32),
        ktab=v((2, nh, span, 128), F32),
        qtab=v((2, nh, span, 128), F32),
        ctab=v((2, nh, CT, 128), F32),
        fade=v((2, nh, 8, DV), F32),
        mask=v((nh, span, span), F32),
        q=v((nh, span, DK), BF16),
        qab=v((nh, span, 2 * DK), BF16),
        k=v((nh, span, DK), BF16),
        v=v((span, nh * DV), BF16),
        ck=v((nh, CT, DK), BF16),
        cv=v((CT, nh * DV), BF16),
        g=v((span, nh * DV), F32),
        ret=v((nh, span, DV), F32),
        gated=v((nh, span, DV), BF16),
        loc=v((2, nh * DK, DV), F32),
        base=v((2, nh * DK, DV), F32),
        st_in=v((2, nh * DK, DV), BF16),
        st_out=v((2, nh * DK, DV), BF16),
        ent=v((nh, 2 * DK, DV), BF16),
        acc=v((span, D), F32),
        part=v((NC, T, R, W), BF16),
        p1=v((NC, X - 1, R, W), BF16),
        p2=v((NC, R, W), BF16),
        xs=v((NC, X - 1, R, W), BF16),
        xr=v((NC, X - 1, R, W), BF16),
        load_sem=DMA((15,)),
        m_send=DMA((2,)),
        m_recv=DMA((2,)),
        lat_send=DMA((1,)),
        lat_recv=DMA((X - 1, pieces)),
        lat_part=DMA((1,)),
        lat_fwd=DMA((X - 1,)),
        ctx_send=DMA((1,)),
        ctx_recv=DMA((2,)),
        st_send=DMA((2,)),
        st_recv=DMA((2, n)),
        out_send=DMA((1,)),
        p1_recv=DMA((NC, X - 1)),
        p2_recv=DMA((1,)),
        x_recv=DMA((NC, X - 1)),
    )
    VMEM = pl.BlockSpec(memory_space=pltpu.VMEM)
    ANY = pl.BlockSpec(memory_space=pl.ANY)
    return pl.pallas_call(
        functools.partial(kernel, S, T, tuple(scratch)),
        out_shape=pltpu.VMEM((R, D), BF16),
        in_specs=[ANY] * 15,
        out_specs=VMEM,
        scratch_shapes=list(scratch.values()),
        compiler_params=pltpu.CompilerParams(
            collective_id=0, has_side_effects=True, vmem_limit_bytes=60 * 1024 * 1024
        ),
    )(
        latent,
        cond.reshape(Mr // 128, 128),
        context_cond.reshape(Mr // 128, 128),
        context,
        norm_gain.reshape(GD, 128),
        mod_shift,
        mod_scale,
        mod_gate,
        w_query,
        w_key,
        w_value,
        w_gate,
        w_out,
        decay_rate,
        context_gain,
    )


def solution(mesh):
    return jax.shard_map(
        functools.partial(body, mesh.shape["sp"], mesh.shape["tp"]),
        mesh=mesh,
        in_specs=(
            P(("grp", "sp", "tp"), None),
            P(("grp", "sp")),
            P(("grp", "sp"), None),
            P("sp"),
            P(),
            P("sp", "tp"),
            P("sp", "tp"),
            P("sp", "tp"),
            P(None, "tp"),
            P(None, "tp"),
            P(None, "tp"),
            P(None, "tp"),
            P("tp", None),
            P(None, "tp"),
            P("tp"),
        ),
        out_specs=P(("grp", "sp", "tp"), None),
        check_vma=False,
    )
```

```python
import functools
import math
from types import SimpleNamespace

import jax
import jax.numpy as jnp
from jax import lax
from jax.experimental import pallas as pl
from jax.experimental.pallas import tpu as pltpu
from jax.sharding import PartitionSpec as P

DK = 256
GRID_W = 128
TILE = 256
PIECE = 16
EARLY = 1
OWN = 1
CHUNK = 32
LAG = (6, 4)
PRE = 1
SPARE = (1, 1, 1, 2)
NC = 2
DIRECT = 256
norm_eps = 1e-06
rope_base = 10000.0
MESH = pl.DeviceIdType.MESH
F32, BF16 = jnp.float32, jnp.bfloat16


def dot(a, b):
    return jnp.dot(a, b, preferred_element_type=F32)


def dot_tn(a, b):
    return lax.dot_general(a, b, (((0,), (0,)), ((), ())), preferred_element_type=F32)


def dot_nt(a, b):
    return lax.dot_general(a, b, (((1,), (1,)), ((), ())), preferred_element_type=F32)


def remote(src, dst, send, recv, where):
    return pltpu.make_async_remote_copy(
        src_ref=src, dst_ref=dst, send_sem=send, recv_sem=recv, device_id=where, device_id_type=MESH
    )


def rows_of(start, size):
    return pl.ds(pl.multiple_of(start, size), size)


def cols(j, size):
    return pl.ds(pl.multiple_of(j * size, size), size)


def drain(ref, sem):
    pltpu.make_async_copy(ref, ref, sem).wait()


def tiled(x, count):
    return jnp.concatenate([x] * count, axis=0) if count > 1 else x


def kernel(S, T, names, *refs):
    (
        latent,
        cond,
        context_cond,
        context,
        norm_gain,
        mod_shift,
        mod_scale,
        mod_gate,
        w_query,
        w_key,
        w_value,
        w_gate,
        w_out,
        decay_in,
        gain_in,
        out,
    ) = refs[:16]
    r = SimpleNamespace(**dict(zip(names, refs[16:])))

    sp, tp = lax.axis_index("sp"), lax.axis_index("tp")
    R, D = latent.shape
    Cr = context.shape[0]
    half = Cr // 2
    CT = Cr * S
    span = R * T
    nh = w_query.shape[1] // DK
    DV = w_value.shape[1] // nh
    Mr, Mc = mod_shift.shape
    G, GD = Mc // 128, D // 128
    X = T // 2
    pieces = R // PIECE
    chip, core = tp // 2, lax.rem(tp, 2)
    partner = tp + 1 - 2 * core
    is_end = jnp.logical_or(sp == 0, sp == S - 1)
    V = (D - DIRECT) // NC
    per_head = DK // CHUNK
    n = nh * per_head
    hop = (sp, S - 1 - sp)
    after = (sp + 1, sp - 1)
    before = (sp - 1, sp + 1)
    sp_peers = [lax.rem(sp + k, S) for k in range(1, S)]
    others = [lax.rem(chip + k, X) for k in range(1, X)]
    origins = [lax.rem(chip + X - k, X) for k in range(1, X)]
    peers = [
        (lax.rem(sp + i, S), lax.rem(tp + j, T)) for i in range(S) for j in range(T) if i or j
    ]

    barrier = pltpu.get_barrier_semaphore()
    for a, b in peers:
        pl.semaphore_signal(
            barrier, inc=1, device_id={"sp": a, "tp": b}, device_id_type=MESH
        )

    own = rows_of(tp * R, R)
    pairs = [
        (latent, r.x_all.at[own]),
        (cond, r.cond),
        (context_cond, r.ccond),
        (mod_shift, r.m_shift),
        (mod_scale, r.m_scale),
        (mod_gate, r.m_gate),
        (decay_in, r.decay),
        (gain_in, r.gain),
        (norm_gain, r.ngain),
        (context, r.c_all.at[rows_of(sp * Cr, Cr)]),
        (w_key, r.vk),
        (w_value, r.vv),
        (w_query, r.vq),
        (w_gate, r.vg),
        (w_out, r.vo),
    ]
    loads = [
        pltpu.make_async_copy(src, dst, r.load_sem.at[i]) for i, (src, dst) in enumerate(pairs)
    ]
    for copy in loads:
        copy.start()

    def lat_copy(owner, p, to, sem):
        place = rows_of(owner * R + p * PIECE, PIECE)
        return remote(r.x_all.at[place], r.x_all.at[place], r.lat_send.at[0], sem, {"tp": to})

    def lat_whole(owner, to, sem):
        place = rows_of(owner * R, R)
        return remote(r.x_all.at[place], r.x_all.at[place], r.lat_send.at[0], sem, {"tp": to})

    def lat_pieces(begin, end):
        for p in range(begin, end):
            for k, o in enumerate(others):
                lat_copy(tp, p, 2 * o + core, r.lat_recv.at[k, p]).start()

    def greet():
        loads[0].wait()
        pl.semaphore_wait(barrier, len(peers))
        lat_pieces(0, EARLY)

    late = 2 * sp >= S
    pl.when(late)(greet)

    for copy in loads[1:3]:
        copy.wait()

    def silu_row(ref):
        v = ref[...].astype(F32)
        v = v / (1.0 + jnp.exp(-v))
        return jnp.concatenate([v[g : g + 1, :] for g in range(Mr // 128)], axis=1)

    rows = jnp.concatenate(
        [silu_row(r.cond), silu_row(r.ccond), jnp.zeros((14, Mr), F32)], axis=0
    ).astype(BF16)
    loads[3].wait()
    shift_part = dot(rows, r.m_shift[...])
    loads[4].wait()
    scale_part = dot(rows, r.m_scale[...])

    me = sp * T + tp

    def lanes(x, row, g):
        return x[row : row + 1, g * 128 : (g + 1) * 128]

    for g in range(G):
        r.m1[me, g : g + 1, :] = lanes(shift_part, 0, g)
        r.m1[me, G + g : G + g + 1, :] = lanes(scale_part, 0, g)

    def m_copy(ref, i, to, slot=me):
        return remote(
            ref.at[slot],
            ref.at[slot],
            r.m_send.at[i],
            r.m_recv.at[i],
            {"sp": to[0], "tp": to[1]},
        )

    sp_all = [sp] + sp_peers
    near = [(a, b) for a in sp_all for b in (tp, partner) if a is not sp or b is not tp]
    across_x = [(a, 2 * o + core) for a in sp_all for o in others]

    def ctx_copy(owner, part_core, recv, where):
        place = rows_of(owner * Cr + part_core * half, half)
        return remote(r.c_all.at[place], r.c_all.at[place], r.ctx_send.at[0], recv, where)

    pl.when(jnp.logical_not(late))(greet)

    for to in across_x:
        m_copy(r.m1, 2, to).start()
    for to in near:
        m_copy(r.m1, 0, to).start()
    lat_pieces(EARLY, pieces)
    lat_whole(tp, partner, r.lat_part.at[0]).start()

    loads[5].wait()
    gate_part = dot(rows, r.m_gate[...])
    for g in range(G):
        r.m2[me, g : g + 1, :] = lanes(shift_part, 1, g)
        r.m2[me, G + g : G + g + 1, :] = lanes(scale_part, 1, g)
        r.m2[me, 2 * G + g : 2 * G + g + 1, :] = lanes(gate_part, 0, g)
    loads[9].wait()
    for to in peers:
        m_copy(r.m2, 1, to).start()
    for to in sp_peers:
        ctx_copy(sp, core, r.ctx_recv.at[0], {"sp": to}).start()

    F = DK // 4
    pos = (lax.broadcasted_iota(jnp.int32, (span, 2 * F), 0) + sp * span).astype(F32)
    lane = lax.broadcasted_iota(jnp.int32, (span, 2 * F), 1)
    grid_row = jnp.floor(pos * (1.0 / GRID_W))
    grid_col = pos - grid_row * GRID_W
    freq = jnp.where(lane < F, lane, lane - F).astype(F32)
    angle = jnp.where(lane < F, grid_row, grid_col) * jnp.exp(freq * (-math.log(rope_base) / F))
    r.cos_t[...] = jnp.cos(angle)
    r.sin_t[...] = jnp.sin(angle)

    for copy in loads[6:9]:
        copy.wait()

    def decay_tables(h, _):
        a, b = r.decay[0, h], r.decay[1, h]
        place = lax.broadcasted_iota(jnp.int32, (span, 128), 0).astype(F32)
        r.ktab[0, h] = jnp.exp(-a * (span - 1.0 - place))
        r.ktab[1, h] = jnp.exp(-b * place)
        r.qtab[0, h] = jnp.exp(-a * (place + 1.0))
        r.qtab[1, h] = jnp.exp(-b * (span - place))
        far = lax.broadcasted_iota(jnp.int32, (CT, 128), 0).astype(F32)
        r.ctab[0, h] = jnp.exp(-a * (CT - 1.0 - far))
        r.ctab[1, h] = jnp.exp(-b * far)
        for d, rate in enumerate((a, b)):
            r.fade[d, h] = jnp.exp(jnp.full((8, DV), -rate * span, F32))
        gap = (
            lax.broadcasted_iota(jnp.int32, (span, span), 0)
            - lax.broadcasted_iota(jnp.int32, (span, span), 1)
        ).astype(F32)
        mask = jnp.where(gap >= 0, jnp.exp(-a * jnp.maximum(gap, 0.0)), 0.0)
        mask += jnp.where(gap <= 0, jnp.exp(-b * jnp.maximum(-gap, 0.0)), 0.0)
        r.mask[h] = mask
        return 0

    lax.fori_loop(0, nh, decay_tables, 0)

    def stat(src, dst, start, count):
        place = rows_of(start, count)
        x = src[place, :].astype(F32)
        inv = lax.rsqrt(jnp.mean(x * x, axis=-1, keepdims=True) + norm_eps)
        dst[place, :] = jnp.broadcast_to(inv, (count, 128))

    def apply(src, dst, inv, start, count, row):
        place = rows_of(start, count)
        scale = inv[place, :]
        for j in range(GD):
            c = slice(j * 128, (j + 1) * 128)
            mult = tiled(r.mult[row, :, c], count // 8)
            shift = tiled(r.shift[row, :, c], count // 8)
            dst[place, c] = (src[place, c].astype(F32) * scale * mult + shift).astype(BF16)

    def spread(row, source, at_shift, at_scale):
        for t in range(T):
            total = source[t]
            for s in range(1, S):
                total = total + source[s * T + t]
            r.g16[0, t * G : (t + 1) * G, :] = total[at_shift : at_shift + G]
            r.g16[1, t * G : (t + 1) * G, :] = total[at_scale : at_scale + G]
            if row:
                r.g16[2, t * G : (t + 1) * G, :] = total[2 * G : 3 * G]
        r.g16[1] = r.ngain[...].astype(F32) * (1.0 + r.g16[1])
        for j in range(GD):
            c = slice(j * 128, (j + 1) * 128)
            r.shift[row, :, c] = jnp.broadcast_to(r.g16[0, j : j + 1, :], (8, 128))
            r.mult[row, :, c] = jnp.broadcast_to(r.g16[1, j : j + 1, :], (8, 128))
            if row:
                r.gate[:, c] = jnp.broadcast_to(r.g16[2, j : j + 1, :], (8, 128))

    def pass_on(p):
        for k, o in enumerate(origins):
            owner = 2 * o + core
            lat_copy(owner, p, tp, r.lat_recv.at[k, p]).wait_recv()
            lat_copy(owner, p, partner, r.lat_fwd.at[k]).start()

    def rows_done(owner):
        stat(r.x_all, r.inv, owner * R, R)
        apply(r.x_all, r.h, r.inv, owner * R, R, 0)

    scale_k = DK**-0.5

    def rotated(x, place):
        u, w = x[:, : DK // 2], x[:, DK // 2 :]
        c, s = r.cos_t[place, :], r.sin_t[place, :]
        return jnp.concatenate([u * c - w * s, w * c + u * s], axis=1).astype(BF16)

    def st_copy(d, c, to):
        place = rows_of(c * CHUNK, CHUNK)
        return remote(
            r.st_out.at[d, place],
            r.st_in.at[d, place],
            r.st_send.at[d],
            r.st_recv.at[d, c],
            {"sp": to},
        )

    first = jnp.where(2 * sp < S, 0, 1)
    onward = jnp.where(2 * sp < S, sp + 1, sp - 1)

    def wide(x):
        return jnp.concatenate([x] * (DK // 128), axis=1)

    def key_value(h, o):
        place = rows_of(2 * o * R, 2 * R)
        hidden = r.h[place, :]
        keys = dot(hidden, r.vk[:, cols(h, DK)]) * scale_k
        r.k[h, place, :] = rotated(keys, place)
        r.v[place, cols(h, DV)] = dot(hidden, r.vv[:, cols(h, DV)]).astype(BF16)

    def local_state(h, d):
        keys = (r.k[h].astype(F32) * wide(r.ktab[d, h])).astype(BF16)
        r.loc[d, cols(h, DK), :] = dot_tn(keys, r.v[:, cols(h, DV)])

    def own_rows(h, _):
        key_value(h, chip)
        return 0

    def head_states(h, _):
        for o in others:
            key_value(h, o)
        local_state(h, first)

        @pl.when(is_end)
        def _():
            for c in range(per_head):
                place = rows_of(h * DK + c * CHUNK, CHUNK)
                r.st_out[first, place, :] = r.loc[first, place, :].astype(BF16)
                st_copy(first, h * per_head + c, onward).start()

        local_state(h, 1 - first)
        return 0

    stat(r.x_all, r.inv, tp * R, R)
    for p in range(pieces - 2):
        pass_on(p)
    drain(r.m1.at[pl.ds(0, len(across_x))], r.m_recv.at[2])
    for a in sp_all:
        for o in origins:
            m_copy(r.m1, 3, (sp, partner), a * T + 2 * o + core).start()
    drain(r.m1.at[pl.ds(0, len(near))], r.m_recv.at[0])
    drain(r.m1.at[pl.ds(0, len(across_x))], r.m_recv.at[3])
    spread(0, r.m1, 0, G)
    apply(r.x_all, r.h, r.inv, tp * R, R, 0)
    lat_whole(partner, partner, r.lat_part.at[0]).wait_recv()
    rows_done(partner)
    loads[10].wait()
    loads[11].wait()
    for p in range(max(pieces - 2, 0), pieces - 1):
        pass_on(p)
    lax.fori_loop(0, min(nh, OWN), own_rows, 0)
    pass_on(pieces - 1)
    for o in origins:
        rows_done(2 * o + core)
    lax.fori_loop(min(nh, OWN), nh, own_rows, 0)
    for k, o in enumerate(origins):
        owner = 2 * o + 1 - core
        lat_whole(owner, owner, r.lat_fwd.at[k]).wait_recv()
        rows_done(owner)
    lax.fori_loop(0, nh, head_states, 0)

    def relay(d, c):
        st_copy(d, c, before[d]).wait_recv()
        place = rows_of(c * CHUNK, CHUNK)
        fade = r.fade[d, lax.div(c, per_head), 0:1, :]
        r.st_out[d, place, :] = (
            r.st_in[d, place, :].astype(F32) * fade + r.loc[d, place, :]
        ).astype(BF16)
        st_copy(d, c, after[d]).start()

    loads[12].wait()
    q_all = dot(r.h[...], r.vq[...])
    for h in range(nh):
        q = rotated(q_all[:, h * DK : (h + 1) * DK], slice(0, span))
        r.q[h] = q
        qf = q.astype(F32)
        r.qab[h, :, :DK] = (qf * wide(r.qtab[0, h])).astype(BF16)
        r.qab[h, :, DK:] = (qf * wide(r.qtab[1, h])).astype(BF16)
    loads[13].wait()
    loads[14].wait()

    def gate_item(j):
        pre = dot(r.h[...], r.vg[:, cols(j, TILE)])
        r.g[:, cols(j, TILE)] = pre / (1.0 + jnp.exp(-pre))

    def within_item(h):
        weights = (dot_nt(r.q[h], r.k[h]) * r.mask[h]).astype(BF16)
        r.ret[h] = dot(weights, r.v[:, cols(h, DV)])

    def ctx_forward_item(_):
        drain(r.c_all.at[rows_of(0, (S - 1) * half)], r.ctx_recv.at[0])
        for p in sp_peers:
            ctx_copy(p, core, r.ctx_recv.at[1], {"tp": partner}).start()
        drain(r.m2.at[pl.ds(0, len(peers))], r.m_recv.at[1])
        spread(1, r.m2, 0, G)

    def ctx_arrive_item(_):
        drain(r.c_all.at[rows_of(0, (S - 1) * half)], r.ctx_recv.at[1])

    def ctx_norm_item(j):
        stat(r.c_all, r.cinv, j * 64, 64)
        apply(r.c_all, r.hc, r.cinv, j * 64, 64, 1)

    M = min(CT, TILE)

    def ctx_key_item(j):
        place, h = rows_of(lax.div(j, nh) * M, M), lax.rem(j, nh)
        r.ck[h, place, :] = (dot(r.hc[place, :], r.vk[:, cols(h, DK)]) * scale_k).astype(BF16)

    nv = nh * DV // TILE

    def ctx_value_item(j):
        place, t = rows_of(lax.div(j, nv) * M, M), lax.rem(j, nv)
        r.cv[place, cols(t, TILE)] = dot(r.hc[place, :], r.vv[:, cols(t, TILE)]).astype(BF16)

    def ctx_state_item(j):
        h, d = lax.div(j, 2), lax.rem(j, 2)
        keys = (r.ck[h].astype(F32) * wide(r.ctab[d, h])).astype(BF16)
        away = jnp.where(d == 0, hop[0], hop[1]).astype(F32) * span
        weight = jnp.exp(jnp.full((1, DV), -r.decay[d, h] * away, F32)) * r.gain[h]
        r.base[d, cols(h, DK), :] = dot_tn(keys, r.cv[:, cols(h, DV)]) * weight

    items = [
        (nv, gate_item),
        (nh, within_item),
        (SPARE[0], None),
        (1, ctx_forward_item),
        (SPARE[1], None),
        (1, ctx_arrive_item),
        (CT // 64, ctx_norm_item),
        (CT // M * nh, ctx_key_item),
        (SPARE[2], None),
        (CT // M * nv, ctx_value_item),
        (SPARE[3], None),
        (2 * nh, ctx_state_item),
    ]
    total_items = sum(count for count, _ in items)
    inner = jnp.logical_not(is_end)

    def lap(i, _):
        for d in (1, 0):
            c = i - PRE - LAG[d] * (hop[d] - 1)

            @pl.when(jnp.logical_and(inner, jnp.logical_and(c >= 0, c < n)))
            def _():
                relay(d, c)

        start = 0
        for count, run in items:
            if run is not None:

                @pl.when(jnp.logical_and(i >= start, i < start + count))
                def _():
                    run(i - start)

            start += count
        return 0

    lax.fori_loop(0, max(PRE + n + max(LAG) * max(S - 3, 0), total_items), lap, 0)

    def project(h, start, count, place):
        return dot(r.gated[h, rows_of(start, count), :], r.vo[h * DV : (h + 1) * DV, place])

    for h in range(nh):
        for d in range(2):

            @pl.when(hop[d] == 0)
            def _():
                r.ent[h, d * DK : (d + 1) * DK, :] = r.base[d, h * DK : (h + 1) * DK, :].astype(
                    BF16
                )

            @pl.when(hop[d] > 0)
            def _():
                def enter(c, _):
                    @pl.when(hop[d] == S - 1)
                    def _():
                        st_copy(d, h * per_head + c, before[d]).wait_recv()

                    place = rows_of(h * DK + c * CHUNK, CHUNK)
                    r.ent[h, rows_of(d * DK + c * CHUNK, CHUNK), :] = (
                        r.st_in[d, place, :].astype(F32) + r.base[d, place, :]
                    ).astype(BF16)
                    return 0

                lax.fori_loop(0, per_head, enter, 0)

        ret = r.ret[h] + dot(r.qab[h], r.ent[h])
        ret = ret - jnp.mean(ret, axis=-1, keepdims=True)
        ret = ret * lax.rsqrt(jnp.mean(ret * ret, axis=-1, keepdims=True) + norm_eps)
        r.gated[h] = (r.g[:, h * DV : (h + 1) * DV] * ret).astype(BF16)
        if h < nh - 1:

            def gather(c, _):
                place = cols(c, D // 4)
                value = project(h, 0, span, place)
                if h:
                    value = value + r.acc[:, place]
                r.acc[:, place] = value
                return 0

            lax.fori_loop(0, 4, gather, 0)

    def chip_rows(dst, o, place):
        value = project(nh - 1, 2 * o * R, 2 * R, place)
        if nh > 1:
            value = value + r.acc[rows_of(2 * o * R, 2 * R), place]
        value = value.astype(BF16)
        dst[0] = value[:R]
        dst[1] = value[R:]

    strips = [slice(DIRECT + c * V, DIRECT + (c + 1) * V) for c in range(NC)]

    def d_copy(k, o, c):
        return remote(
            r.dpart.at[k, c],
            r.dr.at[k, core],
            r.out_send.at[0],
            r.d_recv.at[0],
            {"tp": 2 * o + c},
        )

    def p1_copy(c, k):
        return remote(
            r.part.at[c, k, 1 - core],
            r.p1.at[c, k],
            r.out_send.at[1],
            r.p1_recv.at[c, k],
            {"tp": partner},
        )

    def x_copy(c, k, o):
        return remote(
            r.xs.at[c, k],
            r.xr.at[c, k],
            r.out_send.at[2],
            r.x_recv.at[c, k],
            {"tp": 2 * o + core},
        )

    def p2_copy(place):
        return remote(
            r.home.at[1 - core, :, place],
            r.p2.at[:, place],
            r.out_send.at[3],
            r.p2_recv.at[0],
            {"tp": partner},
        )

    for k, o in enumerate(others):
        chip_rows(r.dpart.at[k], o, slice(0, DIRECT))
        for c in range(2):
            d_copy(k, o, c).start()
    for c in range(NC):
        for k, o in enumerate(others):
            chip_rows(r.part.at[c, k], o, strips[c])
            p1_copy(c, k).start()
    for c in range(NC):
        for k, o in enumerate(others):
            p1_copy(c, k).wait_recv()
            mine = r.part[c, k, core].astype(F32)
            r.xs[c, k] = (mine + r.p1[c, k].astype(F32)).astype(BF16)
            x_copy(c, k, o).start()
        place = slice(c * (D // NC), (c + 1) * (D // NC))
        chip_rows(r.home.at[:, :, place], chip, slice(place.start, place.stop))
        p2_copy(place).start()

    drain(r.m1.at[pl.ds(0, len(near))], r.m_send.at[0])
    drain(r.m1.at[pl.ds(0, len(across_x))], r.m_send.at[2])
    drain(r.m1.at[pl.ds(0, len(across_x))], r.m_send.at[3])
    drain(r.m2.at[pl.ds(0, len(peers))], r.m_send.at[1])
    drain(r.x_all.at[rows_of(0, (T - 1) * R)], r.lat_send.at[0])
    drain(r.c_all.at[rows_of(0, (S - 1) * Cr)], r.ctx_send.at[0])
    for d in range(2):

        @pl.when(hop[d] < S - 1)
        def _():
            drain(r.st_out.at[d], r.st_send.at[d])

    drain(r.p2, r.p2_recv.at[0])

    def final(place, arrived):
        total = r.home[core, :, place].astype(F32) + r.p2[:, place].astype(F32)
        for piece in arrived:
            total = total + piece.astype(F32)
        mine = r.x_all[own, place].astype(F32)
        out[:, place] = (mine + tiled(r.gate[:, place], R // 8) * total).astype(BF16)

    drain(r.dr, r.d_recv.at[0])
    final(slice(0, DIRECT), [r.dr[k, c] for k in range(X - 1) for c in range(2)])
    for c in range(NC):
        for k, o in enumerate(origins):
            x_copy(c, k, o).wait_recv()
        final(strips[c], [r.xr[c, k] for k in range(X - 1)])
    drain(r.dpart, r.out_send.at[0])
    drain(r.p1, r.out_send.at[1])
    drain(r.xs, r.out_send.at[2])
    drain(r.p2, r.out_send.at[3])


def body(
    S,
    T,
    latent,
    cond,
    context,
    context_cond,
    norm_gain,
    mod_shift,
    mod_scale,
    mod_gate,
    w_query,
    w_key,
    w_value,
    w_gate,
    w_out,
    decay_rate,
    context_gain,
):
    R, D = latent.shape
    Cr = context.shape[0]
    span, CT = R * T, Cr * S
    nh = w_query.shape[1] // DK
    DV = w_value.shape[1] // nh
    Mr, Mc = mod_shift.shape
    G, GD = Mc // 128, D // 128
    X = T // 2
    V = (D - DIRECT) // NC
    n = nh * DK // CHUNK
    pieces = R // PIECE
    v = pltpu.VMEM
    DMA = pltpu.SemaphoreType.DMA
    scratch = dict(
        x_all=v((span, D), BF16),
        c_all=v((CT, D), BF16),
        h=v((span, D), BF16),
        hc=v((CT, D), BF16),
        cond=v((Mr // 128, 128), BF16),
        ccond=v((Mr // 128, 128), BF16),
        ngain=v((GD, 128), BF16),
        decay=pltpu.SMEM(decay_rate.shape, F32),
        gain=pltpu.SMEM(context_gain.shape, F32),
        m_shift=v((Mr, Mc), BF16),
        m_scale=v((Mr, Mc), BF16),
        m_gate=v((Mr, Mc), BF16),
        vq=v(w_query.shape, BF16),
        vk=v(w_key.shape, BF16),
        vv=v(w_value.shape, BF16),
        vg=v(w_gate.shape, BF16),
        vo=v(w_out.shape, BF16),
        m1=v((S * T, 2 * G, 128), F32),
        m2=v((S * T, 3 * G, 128), F32),
        g16=v((3, GD, 128), F32),
        shift=v((2, 8, D), F32),
        mult=v((2, 8, D), F32),
        gate=v((8, D), F32),
        inv=v((span, 128), F32),
        cinv=v((CT, 128), F32),
        cos_t=v((span, DK // 2), F32),
        sin_t=v((span, DK // 2), F32),
        ktab=v((2, nh, span, 128), F32),
        qtab=v((2, nh, span, 128), F32),
        ctab=v((2, nh, CT, 128), F32),
        fade=v((2, nh, 8, DV), F32),
        mask=v((nh, span, span), F32),
        q=v((nh, span, DK), BF16),
        qab=v((nh, span, 2 * DK), BF16),
        k=v((nh, span, DK), BF16),
        v=v((span, nh * DV), BF16),
        ck=v((nh, CT, DK), BF16),
        cv=v((CT, nh * DV), BF16),
        g=v((span, nh * DV), F32),
        ret=v((nh, span, DV), F32),
        gated=v((nh, span, DV), BF16),
        loc=v((2, nh * DK, DV), F32),
        base=v((2, nh * DK, DV), F32),
        st_in=v((2, nh * DK, DV), BF16),
        st_out=v((2, nh * DK, DV), BF16),
        ent=v((nh, 2 * DK, DV), BF16),
        acc=v((span, D), F32),
        dpart=v((X - 1, 2, R, DIRECT), BF16),
        dr=v((X - 1, 2, R, DIRECT), BF16),
        part=v((NC, X - 1, 2, R, V), BF16),
        p1=v((NC, X - 1, R, V), BF16),
        xs=v((NC, X - 1, R, V), BF16),
        xr=v((NC, X - 1, R, V), BF16),
        home=v((2, R, D), BF16),
        p2=v((R, D), BF16),
        load_sem=DMA((15,)),
        m_send=DMA((4,)),
        m_recv=DMA((4,)),
        lat_send=DMA((1,)),
        lat_recv=DMA((X - 1, pieces)),
        lat_part=DMA((1,)),
        lat_fwd=DMA((X - 1,)),
        ctx_send=DMA((1,)),
        ctx_recv=DMA((2,)),
        st_send=DMA((2,)),
        st_recv=DMA((2, n)),
        out_send=DMA((4,)),
        d_recv=DMA((1,)),
        p1_recv=DMA((NC, X - 1)),
        p2_recv=DMA((1,)),
        x_recv=DMA((NC, X - 1)),
    )
    VMEM = pl.BlockSpec(memory_space=pltpu.VMEM)
    ANY = pl.BlockSpec(memory_space=pl.ANY)
    return pl.pallas_call(
        functools.partial(kernel, S, T, tuple(scratch)),
        out_shape=pltpu.VMEM((R, D), BF16),
        in_specs=[ANY] * 15,
        out_specs=VMEM,
        scratch_shapes=list(scratch.values()),
        compiler_params=pltpu.CompilerParams(
            collective_id=0, has_side_effects=True, vmem_limit_bytes=60 * 1024 * 1024
        ),
    )(
        latent,
        cond.reshape(Mr // 128, 128),
        context_cond.reshape(Mr // 128, 128),
        context,
        norm_gain.reshape(GD, 128),
        mod_shift,
        mod_scale,
        mod_gate,
        w_query,
        w_key,
        w_value,
        w_gate,
        w_out,
        decay_rate,
        context_gain,
    )


def solution(mesh):
    return jax.shard_map(
        functools.partial(body, mesh.shape["sp"], mesh.shape["tp"]),
        mesh=mesh,
        in_specs=(
            P(("grp", "sp", "tp"), None),
            P(("grp", "sp")),
            P(("grp", "sp"), None),
            P("sp"),
            P(),
            P("sp", "tp"),
            P("sp", "tp"),
            P("sp", "tp"),
            P(None, "tp"),
            P(None, "tp"),
            P(None, "tp"),
            P(None, "tp"),
            P("tp", None),
            P(None, "tp"),
            P("tp"),
        ),
        out_specs=P(("grp", "sp", "tp"), None),
        check_vma=False,
    )
```

```python
import functools
import math
from types import SimpleNamespace

import jax
import jax.numpy as jnp
from jax import lax
from jax.experimental import pallas as pl
from jax.experimental.pallas import tpu as pltpu
from jax.sharding import PartitionSpec as P

DK = 256
GRID_W = 128
TILE = 256
PIECE = 16
EARLY = 1
OWN = 1
CHUNK = 32
LAG = (6, 4)
PRE = 1
SPARE = (1, 1, 1, 2)
NC = 2
DIRECT = 256
norm_eps = 1e-06
rope_base = 10000.0
MESH = pl.DeviceIdType.MESH
F32, BF16 = jnp.float32, jnp.bfloat16


def dot(a, b):
    return jnp.dot(a, b, preferred_element_type=F32)


def dot_tn(a, b):
    return lax.dot_general(a, b, (((0,), (0,)), ((), ())), preferred_element_type=F32)


def dot_nt(a, b):
    return lax.dot_general(a, b, (((1,), (1,)), ((), ())), preferred_element_type=F32)


def remote(src, dst, send, recv, where):
    return pltpu.make_async_remote_copy(
        src_ref=src, dst_ref=dst, send_sem=send, recv_sem=recv, device_id=where, device_id_type=MESH
    )


def rows_of(start, size):
    return pl.ds(pl.multiple_of(start, size), size)


def cols(j, size):
    return pl.ds(pl.multiple_of(j * size, size), size)


def drain(ref, sem):
    pltpu.make_async_copy(ref, ref, sem).wait()


def tiled(x, count):
    return jnp.concatenate([x] * count, axis=0) if count > 1 else x


def kernel(S, T, names, *refs):
    (
        latent,
        cond,
        context_cond,
        context,
        norm_gain,
        mod_shift,
        mod_scale,
        mod_gate,
        w_query,
        w_key,
        w_value,
        w_gate,
        w_out,
        decay_in,
        gain_in,
        out,
    ) = refs[:16]
    r = SimpleNamespace(**dict(zip(names, refs[16:])))

    sp, tp = lax.axis_index("sp"), lax.axis_index("tp")
    R, D = latent.shape
    Cr = context.shape[0]
    half = Cr // 2
    CT = Cr * S
    span = R * T
    nh = w_query.shape[1] // DK
    DV = w_value.shape[1] // nh
    Mr, Mc = mod_shift.shape
    G, GD = Mc // 128, D // 128
    X = T // 2
    pieces = R // PIECE
    chip, core = tp // 2, lax.rem(tp, 2)
    partner = tp + 1 - 2 * core
    is_end = jnp.logical_or(sp == 0, sp == S - 1)
    V = (D - DIRECT) // NC
    per_head = DK // CHUNK
    n = nh * per_head
    hop = (sp, S - 1 - sp)
    after = (sp + 1, sp - 1)
    before = (sp - 1, sp + 1)
    sp_peers = [lax.rem(sp + k, S) for k in range(1, S)]
    others = [lax.rem(chip + k, X) for k in range(1, X)]
    origins = [lax.rem(chip + X - k, X) for k in range(1, X)]
    peers = [
        (lax.rem(sp + i, S), lax.rem(tp + j, T)) for i in range(S) for j in range(T) if i or j
    ]

    barrier = pltpu.get_barrier_semaphore()
    for a, b in peers:
        pl.semaphore_signal(
            barrier, inc=1, device_id={"sp": a, "tp": b}, device_id_type=MESH
        )

    own = rows_of(tp * R, R)
    pairs = [
        (latent, r.x_all.at[own]),
        (cond, r.cond),
        (context_cond, r.ccond),
        (mod_shift, r.m_shift),
        (mod_scale, r.m_scale),
        (mod_gate, r.m_gate),
        (decay_in, r.decay),
        (gain_in, r.gain),
        (norm_gain, r.ngain),
        (context, r.c_all.at[rows_of(sp * Cr, Cr)]),
        (w_key, r.vk),
        (w_value, r.vv),
        (w_query, r.vq),
        (w_gate, r.vg),
        (w_out, r.vo),
    ]
    loads = [
        pltpu.make_async_copy(src, dst, r.load_sem.at[i]) for i, (src, dst) in enumerate(pairs)
    ]
    for copy in loads:
        copy.start()

    def lat_copy(owner, p, to, sem):
        place = rows_of(owner * R + p * PIECE, PIECE)
        return remote(r.x_all.at[place], r.x_all.at[place], r.lat_send.at[0], sem, {"tp": to})

    def lat_whole(owner, to, sem):
        place = rows_of(owner * R, R)
        return remote(r.x_all.at[place], r.x_all.at[place], r.lat_send.at[0], sem, {"tp": to})

    def lat_pieces(begin, end):
        for p in range(begin, end):
            for k, o in enumerate(others):
                lat_copy(tp, p, 2 * o + core, r.lat_recv.at[k, p]).start()

    def greet():
        loads[0].wait()
        pl.semaphore_wait(barrier, len(peers))
        lat_pieces(0, EARLY)

    late = 2 * sp >= S
    pl.when(late)(greet)

    for copy in loads[1:3]:
        copy.wait()

    def silu_row(ref):
        v = ref[...].astype(F32)
        v = v / (1.0 + jnp.exp(-v))
        return jnp.concatenate([v[g : g + 1, :] for g in range(Mr // 128)], axis=1)

    rows = jnp.concatenate(
        [silu_row(r.cond), silu_row(r.ccond), jnp.zeros((14, Mr), F32)], axis=0
    ).astype(BF16)
    loads[3].wait()
    shift_part = dot(rows, r.m_shift[...])
    loads[4].wait()
    scale_part = dot(rows, r.m_scale[...])

    me = sp * T + tp

    def lanes(x, row, g):
        return x[row : row + 1, g * 128 : (g + 1) * 128]

    for g in range(G):
        r.m1[me, g : g + 1, :] = lanes(shift_part, 0, g)
        r.m1[me, G + g : G + g + 1, :] = lanes(scale_part, 0, g)

    def m_copy(ref, i, to, slot=me):
        return remote(
            ref.at[slot],
            ref.at[slot],
            r.m_send.at[i],
            r.m_recv.at[i],
            {"sp": to[0], "tp": to[1]},
        )

    sp_all = [sp] + sp_peers
    near = [(a, b) for a in sp_all for b in (tp, partner) if a is not sp or b is not tp]
    across_x = [(a, 2 * o + core) for a in sp_all for o in others]

    def ctx_copy(owner, part_core, recv, where):
        place = rows_of(owner * Cr + part_core * half, half)
        return remote(r.c_all.at[place], r.c_all.at[place], r.ctx_send.at[0], recv, where)

    pl.when(jnp.logical_not(late))(greet)

    for to in across_x:
        m_copy(r.m1, 2, to).start()
    for to in near:
        m_copy(r.m1, 0, to).start()
    lat_pieces(EARLY, pieces)
    lat_whole(tp, partner, r.lat_part.at[0]).start()

    loads[5].wait()
    gate_part = dot(rows, r.m_gate[...])
    for g in range(G):
        r.m2[me, g : g + 1, :] = lanes(shift_part, 1, g)
        r.m2[me, G + g : G + g + 1, :] = lanes(scale_part, 1, g)
        r.m2[me, 2 * G + g : 2 * G + g + 1, :] = lanes(gate_part, 0, g)
    loads[9].wait()
    for to in peers:
        m_copy(r.m2, 1, to).start()
    for to in sp_peers:
        ctx_copy(sp, core, r.ctx_recv.at[0], {"sp": to}).start()

    F = DK // 4
    pos = (lax.broadcasted_iota(jnp.int32, (span, 2 * F), 0) + sp * span).astype(F32)
    lane = lax.broadcasted_iota(jnp.int32, (span, 2 * F), 1)
    grid_row = jnp.floor(pos * (1.0 / GRID_W))
    grid_col = pos - grid_row * GRID_W
    freq = jnp.where(lane < F, lane, lane - F).astype(F32)
    angle = jnp.where(lane < F, grid_row, grid_col) * jnp.exp(freq * (-math.log(rope_base) / F))
    r.cos_t[...] = jnp.cos(angle)
    r.sin_t[...] = jnp.sin(angle)

    for copy in loads[6:9]:
        copy.wait()

    def decay_tables(h, _):
        a, b = r.decay[0, h], r.decay[1, h]
        place = lax.broadcasted_iota(jnp.int32, (span, 128), 0).astype(F32)
        r.ktab[0, h] = jnp.exp(-a * (span - 1.0 - place))
        r.ktab[1, h] = jnp.exp(-b * place)
        r.qtab[0, h] = jnp.exp(-a * (place + 1.0))
        r.qtab[1, h] = jnp.exp(-b * (span - place))
        far = lax.broadcasted_iota(jnp.int32, (CT, 128), 0).astype(F32)
        r.ctab[0, h] = jnp.exp(-a * (CT - 1.0 - far))
        r.ctab[1, h] = jnp.exp(-b * far)
        for d, rate in enumerate((a, b)):
            r.fade[d, h] = jnp.exp(jnp.full((8, DV), -rate * span, F32))
        gap = (
            lax.broadcasted_iota(jnp.int32, (span, span), 0)
            - lax.broadcasted_iota(jnp.int32, (span, span), 1)
        ).astype(F32)
        mask = jnp.where(gap >= 0, jnp.exp(-a * jnp.maximum(gap, 0.0)), 0.0)
        mask += jnp.where(gap <= 0, jnp.exp(-b * jnp.maximum(-gap, 0.0)), 0.0)
        r.mask[h] = mask
        return 0

    lax.fori_loop(0, nh, decay_tables, 0)

    def stat(src, dst, start, count):
        place = rows_of(start, count)
        x = src[place, :].astype(F32)
        inv = lax.rsqrt(jnp.mean(x * x, axis=-1, keepdims=True) + norm_eps)
        dst[place, :] = jnp.broadcast_to(inv, (count, 128))

    def apply(src, dst, inv, start, count, row):
        place = rows_of(start, count)
        scale = inv[place, :]
        for j in range(GD):
            c = slice(j * 128, (j + 1) * 128)
            mult = tiled(r.mult[row, :, c], count // 8)
            shift = tiled(r.shift[row, :, c], count // 8)
            dst[place, c] = (src[place, c].astype(F32) * scale * mult + shift).astype(BF16)

    def spread(row, source, at_shift, at_scale):
        for t in range(T):
            total = source[t]
            for s in range(1, S):
                total = total + source[s * T + t]
            r.g16[0, t * G : (t + 1) * G, :] = total[at_shift : at_shift + G]
            r.g16[1, t * G : (t + 1) * G, :] = total[at_scale : at_scale + G]
            if row:
                r.g16[2, t * G : (t + 1) * G, :] = total[2 * G : 3 * G]
        r.g16[1] = r.ngain[...].astype(F32) * (1.0 + r.g16[1])
        for j in range(GD):
            c = slice(j * 128, (j + 1) * 128)
            r.shift[row, :, c] = jnp.broadcast_to(r.g16[0, j : j + 1, :], (8, 128))
            r.mult[row, :, c] = jnp.broadcast_to(r.g16[1, j : j + 1, :], (8, 128))
            if row:
                r.gate[:, c] = jnp.broadcast_to(r.g16[2, j : j + 1, :], (8, 128))

    def pass_on(p):
        for k, o in enumerate(origins):
            owner = 2 * o + core
            lat_copy(owner, p, tp, r.lat_recv.at[k, p]).wait_recv()
            lat_copy(owner, p, partner, r.lat_fwd.at[k]).start()

    def rows_done(owner):
        stat(r.x_all, r.inv, owner * R, R)
        apply(r.x_all, r.h, r.inv, owner * R, R, 0)

    scale_k = DK**-0.5

    def rotated(x, place):
        u, w = x[:, : DK // 2], x[:, DK // 2 :]
        c, s = r.cos_t[place, :], r.sin_t[place, :]
        return jnp.concatenate([u * c - w * s, w * c + u * s], axis=1).astype(BF16)

    def st_copy(d, c, to):
        place = rows_of(c * CHUNK, CHUNK)
        return remote(
            r.st_out.at[d, place],
            r.st_in.at[d, place],
            r.st_send.at[d],
            r.st_recv.at[d, c],
            {"sp": to},
        )

    first = jnp.where(2 * sp < S, 0, 1)
    onward = jnp.where(2 * sp < S, sp + 1, sp - 1)

    def wide(x):
        return jnp.concatenate([x] * (DK // 128), axis=1)

    def key_value(h, o):
        place = rows_of(2 * o * R, 2 * R)
        hidden = r.h[place, :]
        keys = dot(hidden, r.vk[:, cols(h, DK)]) * scale_k
        r.k[h, place, :] = rotated(keys, place)
        r.v[place, cols(h, DV)] = dot(hidden, r.vv[:, cols(h, DV)]).astype(BF16)

    def local_state(h, d):
        keys = (r.k[h].astype(F32) * wide(r.ktab[d, h])).astype(BF16)
        r.loc[d, cols(h, DK), :] = dot_tn(keys, r.v[:, cols(h, DV)])

    def own_rows(h, _):
        key_value(h, chip)
        return 0

    def head_states(h, _):
        for o in others:
            key_value(h, o)
        local_state(h, first)

        @pl.when(is_end)
        def _():
            for c in range(per_head):
                place = rows_of(h * DK + c * CHUNK, CHUNK)
                r.st_out[first, place, :] = r.loc[first, place, :].astype(BF16)
                st_copy(first, h * per_head + c, onward).start()

        local_state(h, 1 - first)
        return 0

    stat(r.x_all, r.inv, tp * R, R)
    for p in range(pieces - 2):
        pass_on(p)
    drain(r.m1.at[pl.ds(0, len(across_x))], r.m_recv.at[2])
    for a in sp_all:
        for o in origins:
            m_copy(r.m1, 3, (sp, partner), a * T + 2 * o + core).start()
    drain(r.m1.at[pl.ds(0, len(near))], r.m_recv.at[0])
    drain(r.m1.at[pl.ds(0, len(across_x))], r.m_recv.at[3])
    spread(0, r.m1, 0, G)
    apply(r.x_all, r.h, r.inv, tp * R, R, 0)
    lat_whole(partner, partner, r.lat_part.at[0]).wait_recv()
    rows_done(partner)
    loads[10].wait()
    loads[11].wait()
    for p in range(max(pieces - 2, 0), pieces - 1):
        pass_on(p)
    lax.fori_loop(0, min(nh, OWN), own_rows, 0)
    pass_on(pieces - 1)
    for o in origins:
        rows_done(2 * o + core)
    lax.fori_loop(min(nh, OWN), nh, own_rows, 0)
    for k, o in enumerate(origins):
        owner = 2 * o + 1 - core
        lat_whole(owner, owner, r.lat_fwd.at[k]).wait_recv()
        rows_done(owner)
    lax.fori_loop(0, nh, head_states, 0)

    def relay(d, c):
        st_copy(d, c, before[d]).wait_recv()
        place = rows_of(c * CHUNK, CHUNK)
        fade = r.fade[d, lax.div(c, per_head), 0:1, :]
        r.st_out[d, place, :] = (
            r.st_in[d, place, :].astype(F32) * fade + r.loc[d, place, :]
        ).astype(BF16)
        st_copy(d, c, after[d]).start()

    loads[12].wait()
    q_all = dot(r.h[...], r.vq[...])
    for h in range(nh):
        q = rotated(q_all[:, h * DK : (h + 1) * DK], slice(0, span))
        r.q[h] = q
        qf = q.astype(F32)
        r.qab[h, :, :DK] = (qf * wide(r.qtab[0, h])).astype(BF16)
        r.qab[h, :, DK:] = (qf * wide(r.qtab[1, h])).astype(BF16)
    loads[13].wait()
    loads[14].wait()

    def gate_item(j):
        pre = dot(r.h[...], r.vg[:, cols(j, TILE)])
        r.g[:, cols(j, TILE)] = pre / (1.0 + jnp.exp(-pre))

    def within_item(h):
        weights = (dot_nt(r.q[h], r.k[h]) * r.mask[h]).astype(BF16)
        r.ret[h] = dot(weights, r.v[:, cols(h, DV)])

    def ctx_forward_item(_):
        drain(r.c_all.at[rows_of(0, (S - 1) * half)], r.ctx_recv.at[0])
        for p in sp_peers:
            ctx_copy(p, core, r.ctx_recv.at[1], {"tp": partner}).start()
        drain(r.m2.at[pl.ds(0, len(peers))], r.m_recv.at[1])
        spread(1, r.m2, 0, G)

    def ctx_arrive_item(_):
        drain(r.c_all.at[rows_of(0, (S - 1) * half)], r.ctx_recv.at[1])

    def ctx_norm_item(j):
        stat(r.c_all, r.cinv, j * 64, 64)
        apply(r.c_all, r.hc, r.cinv, j * 64, 64, 1)

    M = min(CT, TILE)

    def ctx_key_item(j):
        place, h = rows_of(lax.div(j, nh) * M, M), lax.rem(j, nh)
        r.ck[h, place, :] = (dot(r.hc[place, :], r.vk[:, cols(h, DK)]) * scale_k).astype(BF16)

    nv = nh * DV // TILE

    def ctx_value_item(j):
        place, t = rows_of(lax.div(j, nv) * M, M), lax.rem(j, nv)
        r.cv[place, cols(t, TILE)] = dot(r.hc[place, :], r.vv[:, cols(t, TILE)]).astype(BF16)

    def ctx_state_item(j):
        h, d = lax.div(j, 2), lax.rem(j, 2)
        keys = (r.ck[h].astype(F32) * wide(r.ctab[d, h])).astype(BF16)
        away = jnp.where(d == 0, hop[0], hop[1]).astype(F32) * span
        weight = jnp.exp(jnp.full((1, DV), -r.decay[d, h] * away, F32)) * r.gain[h]
        r.base[d, cols(h, DK), :] = dot_tn(keys, r.cv[:, cols(h, DV)]) * weight

    items = [
        (nv, gate_item),
        (nh, within_item),
        (SPARE[0], None),
        (1, ctx_forward_item),
        (SPARE[1], None),
        (1, ctx_arrive_item),
        (CT // 64, ctx_norm_item),
        (CT // M * nh, ctx_key_item),
        (SPARE[2], None),
        (CT // M * nv, ctx_value_item),
        (SPARE[3], None),
        (2 * nh, ctx_state_item),
    ]
    total_items = sum(count for count, _ in items)
    inner = jnp.logical_not(is_end)

    def lap(i, _):
        for d in (1, 0):
            c = i - PRE - LAG[d] * (hop[d] - 1)

            @pl.when(jnp.logical_and(inner, jnp.logical_and(c >= 0, c < n)))
            def _():
                relay(d, c)

        start = 0
        for count, run in items:
            if run is not None:

                @pl.when(jnp.logical_and(i >= start, i < start + count))
                def _():
                    run(i - start)

            start += count
        return 0

    lax.fori_loop(0, max(PRE + n + max(LAG) * max(S - 3, 0), total_items), lap, 0)

    def project(h, start, count, place):
        return dot(r.gated[h, rows_of(start, count), :], r.vo[h * DV : (h + 1) * DV, place])

    for h in range(nh):
        for d in range(2):

            @pl.when(hop[d] == 0)
            def _():
                r.ent[h, d * DK : (d + 1) * DK, :] = r.base[d, h * DK : (h + 1) * DK, :].astype(
                    BF16
                )

            @pl.when(hop[d] > 0)
            def _():
                def enter(c, _):
                    @pl.when(hop[d] == S - 1)
                    def _():
                        st_copy(d, h * per_head + c, before[d]).wait_recv()

                    place = rows_of(h * DK + c * CHUNK, CHUNK)
                    r.ent[h, rows_of(d * DK + c * CHUNK, CHUNK), :] = (
                        r.st_in[d, place, :].astype(F32) + r.base[d, place, :]
                    ).astype(BF16)
                    return 0

                lax.fori_loop(0, per_head, enter, 0)

            if d == 0:
                r.ret[h] = r.ret[h] + dot(r.qab[h, :, :DK], r.ent[h, :DK])

        ret = r.ret[h] + dot(r.qab[h, :, DK:], r.ent[h, DK:])
        ret = ret - jnp.mean(ret, axis=-1, keepdims=True)
        ret = ret * lax.rsqrt(jnp.mean(ret * ret, axis=-1, keepdims=True) + norm_eps)
        r.gated[h] = (r.g[:, h * DV : (h + 1) * DV] * ret).astype(BF16)
        if h < nh - 1:

            def gather(c, _):
                place = cols(c, D // 4)
                value = project(h, 0, span, place)
                if h:
                    value = value + r.acc[:, place]
                r.acc[:, place] = value
                return 0

            lax.fori_loop(0, 4, gather, 0)

    def chip_rows(dst, o, place):
        value = project(nh - 1, 2 * o * R, 2 * R, place)
        if nh > 1:
            value = value + r.acc[rows_of(2 * o * R, 2 * R), place]
        value = value.astype(BF16)
        dst[0] = value[:R]
        dst[1] = value[R:]

    strips = [slice(DIRECT + c * V, DIRECT + (c + 1) * V) for c in range(NC)]

    def d_copy(k, o, c):
        return remote(
            r.dpart.at[k, c],
            r.dr.at[k, core],
            r.out_send.at[0],
            r.d_recv.at[0],
            {"tp": 2 * o + c},
        )

    def p1_copy(c, k):
        return remote(
            r.part.at[c, k, 1 - core],
            r.p1.at[c, k],
            r.out_send.at[1],
            r.p1_recv.at[c, k],
            {"tp": partner},
        )

    def x_copy(c, k, o):
        return remote(
            r.xs.at[c, k],
            r.xr.at[c, k],
            r.out_send.at[2],
            r.x_recv.at[c, k],
            {"tp": 2 * o + core},
        )

    def p2_copy(place):
        return remote(
            r.home.at[1 - core, :, place],
            r.p2.at[:, place],
            r.out_send.at[3],
            r.p2_recv.at[0],
            {"tp": partner},
        )

    for k, o in enumerate(others):
        chip_rows(r.dpart.at[k], o, slice(0, DIRECT))
        for c in range(2):
            d_copy(k, o, c).start()
    for c in range(NC):
        for k, o in enumerate(others):
            chip_rows(r.part.at[c, k], o, strips[c])
            p1_copy(c, k).start()
    for c in range(NC):
        for k, o in enumerate(others):
            p1_copy(c, k).wait_recv()
            mine = r.part[c, k, core].astype(F32)
            r.xs[c, k] = (mine + r.p1[c, k].astype(F32)).astype(BF16)
            x_copy(c, k, o).start()
        place = slice(c * (D // NC), (c + 1) * (D // NC))
        chip_rows(r.home.at[:, :, place], chip, slice(place.start, place.stop))
        p2_copy(place).start()

    drain(r.m1.at[pl.ds(0, len(near))], r.m_send.at[0])
    drain(r.m1.at[pl.ds(0, len(across_x))], r.m_send.at[2])
    drain(r.m1.at[pl.ds(0, len(across_x))], r.m_send.at[3])
    drain(r.m2.at[pl.ds(0, len(peers))], r.m_send.at[1])
    drain(r.x_all.at[rows_of(0, (T - 1) * R)], r.lat_send.at[0])
    drain(r.c_all.at[rows_of(0, (S - 1) * Cr)], r.ctx_send.at[0])
    for d in range(2):

        @pl.when(hop[d] < S - 1)
        def _():
            drain(r.st_out.at[d], r.st_send.at[d])

    drain(r.p2, r.p2_recv.at[0])

    def final(place, arrived):
        total = r.home[core, :, place].astype(F32) + r.p2[:, place].astype(F32)
        for piece in arrived:
            total = total + piece.astype(F32)
        mine = r.x_all[own, place].astype(F32)
        out[:, place] = (mine + tiled(r.gate[:, place], R // 8) * total).astype(BF16)

    drain(r.dr, r.d_recv.at[0])
    final(slice(0, DIRECT), [r.dr[k, c] for k in range(X - 1) for c in range(2)])
    for c in range(NC):
        for k, o in enumerate(origins):
            x_copy(c, k, o).wait_recv()
        final(strips[c], [r.xr[c, k] for k in range(X - 1)])
    drain(r.dpart, r.out_send.at[0])
    drain(r.p1, r.out_send.at[1])
    drain(r.xs, r.out_send.at[2])
    drain(r.p2, r.out_send.at[3])


def body(
    S,
    T,
    latent,
    cond,
    context,
    context_cond,
    norm_gain,
    mod_shift,
    mod_scale,
    mod_gate,
    w_query,
    w_key,
    w_value,
    w_gate,
    w_out,
    decay_rate,
    context_gain,
):
    R, D = latent.shape
    Cr = context.shape[0]
    span, CT = R * T, Cr * S
    nh = w_query.shape[1] // DK
    DV = w_value.shape[1] // nh
    Mr, Mc = mod_shift.shape
    G, GD = Mc // 128, D // 128
    X = T // 2
    V = (D - DIRECT) // NC
    n = nh * DK // CHUNK
    pieces = R // PIECE
    v = pltpu.VMEM
    DMA = pltpu.SemaphoreType.DMA
    scratch = dict(
        x_all=v((span, D), BF16),
        c_all=v((CT, D), BF16),
        h=v((span, D), BF16),
        hc=v((CT, D), BF16),
        cond=v((Mr // 128, 128), BF16),
        ccond=v((Mr // 128, 128), BF16),
        ngain=v((GD, 128), BF16),
        decay=pltpu.SMEM(decay_rate.shape, F32),
        gain=pltpu.SMEM(context_gain.shape, F32),
        m_shift=v((Mr, Mc), BF16),
        m_scale=v((Mr, Mc), BF16),
        m_gate=v((Mr, Mc), BF16),
        vq=v(w_query.shape, BF16),
        vk=v(w_key.shape, BF16),
        vv=v(w_value.shape, BF16),
        vg=v(w_gate.shape, BF16),
        vo=v(w_out.shape, BF16),
        m1=v((S * T, 2 * G, 128), F32),
        m2=v((S * T, 3 * G, 128), F32),
        g16=v((3, GD, 128), F32),
        shift=v((2, 8, D), F32),
        mult=v((2, 8, D), F32),
        gate=v((8, D), F32),
        inv=v((span, 128), F32),
        cinv=v((CT, 128), F32),
        cos_t=v((span, DK // 2), F32),
        sin_t=v((span, DK // 2), F32),
        ktab=v((2, nh, span, 128), F32),
        qtab=v((2, nh, span, 128), F32),
        ctab=v((2, nh, CT, 128), F32),
        fade=v((2, nh, 8, DV), F32),
        mask=v((nh, span, span), F32),
        q=v((nh, span, DK), BF16),
        qab=v((nh, span, 2 * DK), BF16),
        k=v((nh, span, DK), BF16),
        v=v((span, nh * DV), BF16),
        ck=v((nh, CT, DK), BF16),
        cv=v((CT, nh * DV), BF16),
        g=v((span, nh * DV), F32),
        ret=v((nh, span, DV), F32),
        gated=v((nh, span, DV), BF16),
        loc=v((2, nh * DK, DV), F32),
        base=v((2, nh * DK, DV), F32),
        st_in=v((2, nh * DK, DV), BF16),
        st_out=v((2, nh * DK, DV), BF16),
        ent=v((nh, 2 * DK, DV), BF16),
        acc=v((span, D), F32),
        dpart=v((X - 1, 2, R, DIRECT), BF16),
        dr=v((X - 1, 2, R, DIRECT), BF16),
        part=v((NC, X - 1, 2, R, V), BF16),
        p1=v((NC, X - 1, R, V), BF16),
        xs=v((NC, X - 1, R, V), BF16),
        xr=v((NC, X - 1, R, V), BF16),
        home=v((2, R, D), BF16),
        p2=v((R, D), BF16),
        load_sem=DMA((15,)),
        m_send=DMA((4,)),
        m_recv=DMA((4,)),
        lat_send=DMA((1,)),
        lat_recv=DMA((X - 1, pieces)),
        lat_part=DMA((1,)),
        lat_fwd=DMA((X - 1,)),
        ctx_send=DMA((1,)),
        ctx_recv=DMA((2,)),
        st_send=DMA((2,)),
        st_recv=DMA((2, n)),
        out_send=DMA((4,)),
        d_recv=DMA((1,)),
        p1_recv=DMA((NC, X - 1)),
        p2_recv=DMA((1,)),
        x_recv=DMA((NC, X - 1)),
    )
    VMEM = pl.BlockSpec(memory_space=pltpu.VMEM)
    ANY = pl.BlockSpec(memory_space=pl.ANY)
    return pl.pallas_call(
        functools.partial(kernel, S, T, tuple(scratch)),
        out_shape=pltpu.VMEM((R, D), BF16),
        in_specs=[ANY] * 15,
        out_specs=VMEM,
        scratch_shapes=list(scratch.values()),
        compiler_params=pltpu.CompilerParams(
            collective_id=0, has_side_effects=True, vmem_limit_bytes=60 * 1024 * 1024
        ),
    )(
        latent,
        cond.reshape(Mr // 128, 128),
        context_cond.reshape(Mr // 128, 128),
        context,
        norm_gain.reshape(GD, 128),
        mod_shift,
        mod_scale,
        mod_gate,
        w_query,
        w_key,
        w_value,
        w_gate,
        w_out,
        decay_rate,
        context_gain,
    )


def solution(mesh):
    return jax.shard_map(
        functools.partial(body, mesh.shape["sp"], mesh.shape["tp"]),
        mesh=mesh,
        in_specs=(
            P(("grp", "sp", "tp"), None),
            P(("grp", "sp")),
            P(("grp", "sp"), None),
            P("sp"),
            P(),
            P("sp", "tp"),
            P("sp", "tp"),
            P("sp", "tp"),
            P(None, "tp"),
            P(None, "tp"),
            P(None, "tp"),
            P(None, "tp"),
            P("tp", None),
            P(None, "tp"),
            P("tp"),
        ),
        out_specs=P(("grp", "sp", "tp"), None),
        check_vma=False,
    )
```
